256 devices in a mesh: gr: 2 (over z_hi), sp: 16 (over z_lo, y), tp: 8 (over x, core).
Axes of the slice: x: 4, y: 4, z: 8 (z_hi: 2, z_lo: 4; z = z_hi * 4 + z_lo), core: 2. Of those that a mesh axis runs over, the one named last changes fastest.
Arguments:
- tokens: bfloat16 [4, 8192, 2048], P('gr', 'sp'), parts along dimension 0, may hold values from -6 to 6
- key_matrix: bfloat16 [2048, 2048], P(None, 'tp'), may hold values from -0.125 to 0.125
- value_matrix: bfloat16 [2048, 2048], P(None, 'tp'), may hold values from -0.125 to 0.125
- gate_matrix: bfloat16 [2048, 16], replicated, may hold values from -0.125 to 0.125
- decay_matrix: bfloat16 [2048, 16], replicated, may hold values from -0.125 to 0.125
- gate_bias_offset: float32 [16], replicated, may hold values from -8 to 1
- head_log_decay_rate: float32 [16], replicated, may hold values from -12 to -2
- extra_log_decay: float32 [4, 8192, 16], P('gr', 'sp', 'tp'), parts along dimension 0, may hold values from -1 to 0
- next_token_query: bfloat16 [4, 16, 128], P('gr', 'tp'), parts along dimension 0, may hold values from -6 to 6
- next_token_key: bfloat16 [4, 16, 128], P('gr', 'tp'), parts along dimension 0, may hold values from -6 to 6
- next_token_value: bfloat16 [4, 16, 128], P('gr', 'tp'), parts along dimension 0, may hold values from -6 to 6
- next_token_gate: float32 [4, 16], P('gr', 'tp'), parts along dimension 0, may hold values from -2 to 2
- readout_norm_gain: float32 [128], replicated, may hold values from 0.1 to 1.9
Outputs:
- state_cache: bfloat16 [4, 16, 128, 128], P('gr', 'tp', 'sp'), parts along dimension 0
- first_read: bfloat16 [4, 16, 128], P('gr', 'tp'), parts along dimension 0
The draws below stay inside these ranges and needn't reach their ends.
There are 2 independent parts, one for each index of `gr`. The reference program is written for one: setup_inputs(seed, part) draws one part's arguments, and reference() takes and returns one part's arrays. A program takes and returns all parts, laid end to end along the dimension named above; an argument that names none is the same for every part. Nothing has to cross between parts.
All inputs are finite; a program needn't handle non-finite values.
Results may differ from the reference program's by a relative error of at most 0.009.
Values sent between devices are 32-bit elements; how exact they have to be, the bound alone decides.
No kernel may reach another device: no remote copies, remote signals or barrier semaphores. Data moves between devices by JAX's collectives and lax.ppermute only.
A program may use at most 64 MiB of HBM per device.

```python
import math
import jax
import jax.numpy as jnp
from jax import lax

D = 2048
H = 16
DK = 128
BLOCK = 64
GROUP_SEQUENCES = 2
SEG = 512
SEQUENCE_LENGTH = 8192


def head_ranking(key):
    return jax.random.permutation(jax.random.fold_in(key, 101), H)


def draw_head_log_decay_rate(key, part):
    ranking = head_ranking(key)
    slow_mask = ranking < H // 2
    spread = jax.random.uniform(jax.random.fold_in(key, 5), (H,), jnp.float32, -0.4, 0.4)
    slow_rate = math.log(0.5 / (0.7 * SEQUENCE_LENGTH)) + spread
    fast_rate = math.log(1.0 / 28.0) + 0.75 * spread
    return jnp.where(slow_mask, slow_rate, fast_rate).astype(jnp.float32)


def draw_gate_bias_offset(key, part):
    ranking = head_ranking(key)
    slow_mask = ranking < H // 2
    shake = jax.random.uniform(jax.random.fold_in(key, 7), (H,), jnp.float32, -0.5, 0.5)
    slow_shift = math.log(DK / (8.0 * SEQUENCE_LENGTH)) + shake
    fast_shift = 2.0 * shake
    return jnp.where(slow_mask, slow_shift, fast_shift).astype(jnp.float32)


def draw_extra_log_decay(key, part):
    steady_rate = jnp.exp(jax.random.uniform(jax.random.fold_in(key, 11), (GROUP_SEQUENCES, SEQUENCE_LENGTH // SEG, 1, H), jnp.float32, math.log(0.1), 0.0)) / SEQUENCE_LENGTH
    steady_rate = jnp.broadcast_to(steady_rate, (GROUP_SEQUENCES, SEQUENCE_LENGTH // SEG, SEG, H)).reshape(GROUP_SEQUENCES, SEQUENCE_LENGTH, H)
    spike_positions = jax.random.randint(jax.random.fold_in(key, 13), (GROUP_SEQUENCES, 2), 0, SEQUENCE_LENGTH)
    spike_mask = jnp.any(jnp.arange(SEQUENCE_LENGTH)[None, :, None] == spike_positions[:, None, :], axis=-1)
    write_strength = jnp.log(jax.random.uniform(jax.random.fold_in(key, 17), (GROUP_SEQUENCES, SEQUENCE_LENGTH, H), jnp.float32, 0.55, 0.8))
    return (jnp.where(spike_mask[..., None], write_strength, 0.0) - steady_rate).astype(jnp.float32)


def levels(own_key, dims, shards, least, high):
    factor_of = 1.0
    for axis_at, shards_of in shards:
        heights = jax.random.uniform(jax.random.fold_in(jax.random.fold_in(own_key, 6), axis_at), (shards_of,), jnp.float32, least / len(shards), high / len(shards))
        factor_of = factor_of * jnp.repeat(jnp.exp(heights), dims[axis_at] // shards_of).reshape((-1,) + (1,) * (len(dims) - 1 - axis_at))
    return factor_of


def normal_values(stream_key, extent, deviation, reach, cuts=(), kind=jnp.bfloat16):
    gain = levels(stream_key, extent, cuts, -0.22, 0.18) if cuts else 1.0
    result = jax.random.normal(stream_key, extent, jnp.float32) * deviation * gain
    return jnp.minimum(jnp.maximum(result, -reach), reach).astype(kind)


def setup_inputs(seed: int = 0, part: int = 0) -> dict:
    keys = jax.random.split(jax.random.key(seed), 14)
    part_keys = jax.random.split(jax.random.fold_in(keys[13], part), 14)
    tokens = normal_values(part_keys[0], (GROUP_SEQUENCES, SEQUENCE_LENGTH, D), 1.0, 6.0, ((1, 16),))
    key_matrix = normal_values(keys[1], (D, H * DK), D ** -0.5, 0.125, ((1, 8),))
    value_matrix = normal_values(keys[2], (D, H * DK), D ** -0.5, 0.125, ((1, 8),))
    gate_matrix = normal_values(keys[3], (D, H), D ** -0.5, 0.125)
    decay_matrix = normal_values(keys[4], (D, H), D ** -0.5, 0.125)
    gate_bias_offset = draw_gate_bias_offset(jax.random.fold_in(keys[13], 71), part)
    head_log_decay_rate = draw_head_log_decay_rate(jax.random.fold_in(keys[13], 71), part)
    extra_log_decay = draw_extra_log_decay(jax.random.fold_in(jax.random.fold_in(keys[13], part), 71), part)
    next_token_query = normal_values(part_keys[8], (GROUP_SEQUENCES, H, DK), 1.0, 6.0, ((1, 8),))
    next_token_key = normal_values(part_keys[9], (GROUP_SEQUENCES, H, DK), 1.0, 6.0, ((1, 8),))
    next_token_value = normal_values(part_keys[10], (GROUP_SEQUENCES, H, DK), 1.0, 6.0, ((1, 8),))
    next_token_gate = jnp.clip(jax.random.uniform(part_keys[11], (GROUP_SEQUENCES, H), jnp.float32, -2.0, 2.0) * levels(part_keys[11], (GROUP_SEQUENCES, H), ((1, 8),), -0.4, 0.0), -2.0, 2.0)
    readout_norm_gain = jnp.clip(1.0 + 0.18 * jax.random.normal(keys[12], (DK,), jnp.float32), 0.1, 1.9)
    return dict(tokens=tokens, key_matrix=key_matrix, value_matrix=value_matrix, gate_matrix=gate_matrix, decay_matrix=decay_matrix, gate_bias_offset=gate_bias_offset, head_log_decay_rate=head_log_decay_rate, extra_log_decay=extra_log_decay, next_token_query=next_token_query, next_token_key=next_token_key, next_token_value=next_token_value, next_token_gate=next_token_gate, readout_norm_gain=readout_norm_gain)


def unit_rows(array):
    return array * lax.rsqrt(lax.optimization_barrier(jnp.sum(array * array, axis=-1, keepdims=True)) + 1e-06)

def exact_matmul(left, right):
    return jnp.matmul(left, right, precision=lax.Precision.HIGHEST)

def to_blocks(array, block_len):
    seq_count, length, head_count = array.shape[:3]
    tail_dims = array.shape[3:]
    split_view = array.reshape((seq_count, length // block_len, block_len, head_count) + tail_dims)
    axes_order = (1, 0, 3, 2) + tuple(range(4, split_view.ndim))
    return jnp.transpose(split_view, axes_order)

def block_terms(key_rows, value_rows, beta_rows, decay_logarithm):
    block_len = key_rows.shape[-2]
    cumulative = jnp.cumsum(decay_logarithm, axis=-1)
    positions = jnp.arange(block_len)
    inclusive = positions[:, None] >= positions[None, :]
    strictly = positions[:, None] > positions[None, :]
    decay_mat = jnp.exp(jnp.where(inclusive, cumulative[..., :, None] - cumulative[..., None, :], -jnp.inf))
    weighted = key_rows * beta_rows[..., None]
    lower_part = jnp.where(strictly, jnp.einsum('...id,...jd->...ij', weighted, key_rows, precision=lax.Precision.HIGHEST) * decay_mat, 0.0)
    identity = jnp.eye(block_len, dtype=jnp.float32)
    power_term = -lower_part
    inverse = identity + power_term
    for _ in range(block_len.bit_length() - 2):
        power_term = exact_matmul(power_term, power_term)
        inverse = exact_matmul(inverse, identity + power_term)
    fresh_part = exact_matmul(inverse, value_rows * beta_rows[..., None])
    pull_part = exact_matmul(inverse, weighted * jnp.exp(cumulative)[..., None])
    last_cum = cumulative[..., -1:]
    outward = key_rows * jnp.exp(last_cum - cumulative)[..., None]
    carry_decay = jnp.exp(last_cum)
    return (fresh_part, pull_part, outward, carry_decay)

def advance(state_mat, pieces):
    fresh_part, pull_part, outward, carry_decay = pieces
    update = fresh_part - jnp.einsum('shck,shkv->shcv', pull_part, state_mat, precision=lax.Precision.HIGHEST)
    state_mat = state_mat * carry_decay[..., None] + jnp.einsum('shck,shcv->shkv', outward, update, precision=lax.Precision.HIGHEST)
    return (state_mat, None)

def reference(tokens, key_matrix, value_matrix, gate_matrix, decay_matrix, gate_bias_offset, head_log_decay_rate, extra_log_decay, next_token_query, next_token_key, next_token_value, next_token_gate, readout_norm_gain):
    flat = tokens.reshape(GROUP_SEQUENCES * SEQUENCE_LENGTH, D)
    key_proj = jnp.dot(flat, key_matrix, preferred_element_type=jnp.float32)
    value_proj = jnp.dot(flat, value_matrix, preferred_element_type=jnp.float32)
    key_rows = unit_rows(jax.nn.silu(key_proj).reshape(GROUP_SEQUENCES, SEQUENCE_LENGTH, H, DK)).astype(jnp.bfloat16)
    value_rows = jax.nn.silu(value_proj).reshape(GROUP_SEQUENCES, SEQUENCE_LENGTH, H, DK).astype(jnp.bfloat16)
    gate_pre = jnp.dot(flat, gate_matrix, preferred_element_type=jnp.float32).reshape(GROUP_SEQUENCES, SEQUENCE_LENGTH, H)
    decay_logits = jnp.dot(flat, decay_matrix, preferred_element_type=jnp.float32).reshape(GROUP_SEQUENCES, SEQUENCE_LENGTH, H)
    beta_rows = jax.nn.sigmoid(gate_pre + gate_bias_offset)
    decay_logarithm = -jnp.exp(head_log_decay_rate) * jax.nn.softplus(decay_logits) + extra_log_decay
    pieces = block_terms(to_blocks(key_rows.astype(jnp.float32), BLOCK), to_blocks(value_rows.astype(jnp.float32), BLOCK), to_blocks(beta_rows, BLOCK), to_blocks(decay_logarithm, BLOCK))
    start_state = jnp.zeros((GROUP_SEQUENCES, H, DK, DK), jnp.float32)
    final, _ = lax.scan(advance, start_state, pieces)
    query_unit = unit_rows(next_token_query.astype(jnp.float32))
    key_unit = unit_rows(next_token_key.astype(jnp.float32))
    beta_new = jax.nn.sigmoid(next_token_gate)
    value_new = next_token_value.astype(jnp.float32)
    key_read = jnp.einsum('shk,shkv->shv', key_unit, final, precision=lax.Precision.HIGHEST)
    query_read = jnp.einsum('shk,shkv->shv', query_unit, final, precision=lax.Precision.HIGHEST)
    intersection = lax.optimization_barrier(jnp.sum(key_unit * query_unit, axis=-1))
    missing = value_new - key_read
    updated = final + beta_new[..., None, None] * key_unit[..., :, None] * missing[..., None, :]
    read_vec = (query_read + (beta_new * intersection)[..., None] * missing) / math.sqrt(DK)
    normed = read_vec * lax.rsqrt(lax.optimization_barrier(jnp.mean(read_vec * read_vec, axis=-1, keepdims=True)) + 1e-06) * readout_norm_gain
    return (updated.astype(jnp.bfloat16), normed.astype(jnp.bfloat16))
```

```python
import math

import jax
import jax.numpy as jnp
from jax import lax
from jax.experimental import pallas as pl
from jax.experimental.pallas import tpu as pltpu
from jax.sharding import Mesh
from jax.sharding import PartitionSpec as P

SP = ("sp_0", "sp_1")
CH = 128
F32 = jnp.float32
BF16 = jnp.bfloat16
AB = (((1,), (0,)), ((), ()))
ABT = (((1,), (1,)), ((), ()))
ATB = (((0,), (0,)), ((), ()))


def dot1(a, b, dims=AB):
    return lax.dot_general(a.astype(BF16), b.astype(BF16), dims, preferred_element_type=F32)


def split(a):
    hi = a.astype(BF16)
    return hi, (a - hi.astype(F32)).astype(BF16)


def dot3(a, b, dims=AB):
    ah, al = split(a)
    bh, bl = split(b)
    return dot1(ah, bh, dims) + (dot1(ah, bl, dims) + dot1(al, bh, dims))


def iota(shape, dim):
    return lax.broadcasted_iota(jnp.int32, shape, dim)


def unit_rows(a):
    return a * lax.rsqrt(jnp.sum(a * a, axis=-1, keepdims=True) + 1e-06)


def silu(a):
    return a * (1.0 / (1.0 + jnp.exp(-a)))


def inverse_of(m_mat):
    row = iota((CH, CH), 0)
    col = iota((CH, CH), 1)
    eye = jnp.where(row == col, 1.0, 0.0)
    p1 = jnp.where(row // 16 == col // 16, -m_mat, 0.0)
    inv = eye + p1
    p1 = p1.astype(BF16)
    p2 = dot1(p1, p1).astype(BF16)
    both = dot1(p2, jnp.concatenate([p2, inv.astype(BF16)], axis=1))
    inv = inv + both[:, CH:]
    p4 = both[:, :CH].astype(BF16)
    both = dot1(p4, jnp.concatenate([p4, inv.astype(BF16)], axis=1))
    inv = inv + both[:, CH:]
    p8 = both[:, :CH]
    inv = inv + dot1(p8, inv)
    for b in (16, 32, 64):
        lower = [slice(s + b, s + 2 * b) for s in range(0, CH, 2 * b)]
        m_rows = jnp.concatenate(
            [
                jnp.where(col[r, :] // b == (r.start // b - 1), m_mat[r, :], 0.0)
                for r in lower
            ],
            axis=0,
        )
        t_rows = jnp.concatenate([inv[r, :] for r in lower], axis=0)
        y = dot1(m_rows, inv)
        pieces = []
        for g in range(len(lower)):
            part = y[g * b : (g + 1) * b, :]
            pieces += [part, part]
        new_rows = t_rows - dot1(t_rows, jnp.concatenate(pieces, axis=0))
        pieces = []
        for g, r in enumerate(lower):
            pieces += [inv[r.start - b : r.start, :], new_rows[g * b : (g + 1) * b, :]]
        inv = jnp.concatenate(pieces, axis=0)
    return inv


def maps_kernel(
    x_hbm, wk_hbm, wv_hbm, gate_ref, decay_ref, bias_ref, rate_ref, extra_ref,
    o0, o1, o2, o3,
    xbuf, wkbuf, wvbuf, kbuf, vbuf, gsc, dsc, esc, sbuf, sems,
):
    seqs = xbuf.shape[0] // 2
    first_head = lax.axis_index("tp") * 2
    here = lax.axis_index("sp_1")
    tiles, tile, width = xbuf.shape
    copies = []
    for t in range(tiles):
        s, half = divmod(t, tiles // seqs)
        copies.append(
            pltpu.make_async_copy(x_hbm.at[s, pl.ds(half * tile, tile)], xbuf.at[t], sems.at[t])
        )
    wk_copy = pltpu.make_async_copy(wk_hbm, wkbuf, sems.at[tiles])
    wv_copy = pltpu.make_async_copy(wv_hbm, wvbuf, sems.at[tiles + 1])
    wk_copy.start()
    copies[0].start()
    wv_copy.start()
    for c in copies[1:]:
        c.start()
    per_tile = tile // CH
    gates = jnp.concatenate([gate_ref[...], decay_ref[...]], axis=0)
    heads = gate_ref.shape[0]
    pick = iota((heads, tile), 0)
    wk_copy.wait()
    for t in range(tiles):
        copies[t].wait()
        if t == 0:
            wv_copy.wait()
        x = xbuf[t]
        kp = silu(lax.dot_general(x, wkbuf[...], AB, preferred_element_type=F32))
        rows = slice(t * tile, (t + 1) * tile)
        for h in range(2):
            lanes = slice(h * CH, (h + 1) * CH)
            kbuf[rows, lanes] = unit_rows(kp[:, lanes]).astype(BF16)
        vp = silu(lax.dot_general(x, wvbuf[...], AB, preferred_element_type=F32))
        vbuf[rows, :] = vp.astype(BF16)
        gt = lax.dot_general(gates, x, ABT, preferred_element_type=F32)
        for h in range(2):
            mine = pick == first_head + h
            g_row = jnp.sum(jnp.where(mine, gt[:heads], 0.0), axis=0, keepdims=True)
            d_row = jnp.sum(jnp.where(mine, gt[heads:], 0.0), axis=0, keepdims=True)
            for q in range(per_tile):
                r = 2 * (t * per_tile + q) + h
                gsc[r : r + 1, :] = g_row[:, q * CH : (q + 1) * CH]
                dsc[r : r + 1, :] = d_row[:, q * CH : (q + 1) * CH]
    count = gsc.shape[0]
    chunks = count // 2
    per_seq = chunks // seqs
    for m in range(chunks):
        s, n = divmod(m, per_seq)
        esc[2 * m : 2 * m + 2, :] = extra_ref[s, :, n * CH : (n + 1) * CH]
    odd = iota((count, CH), 0) % 2 == 1
    lane = iota((count, CH), 1)
    bias = jnp.where(odd, bias_ref[first_head + 1], bias_ref[first_head])
    rate = jnp.where(odd, rate_ref[first_head + 1], rate_ref[first_head])
    beta = 1.0 / (1.0 + jnp.exp(-(gsc[...] + bias)))
    z = dsc[...]
    soft = jnp.maximum(z, 0.0) + jnp.log1p(jnp.exp(-jnp.abs(z)))
    cum = -jnp.exp(rate) * soft + esc[...]
    d = 1
    while d < CH:
        cum = cum + jnp.where(lane >= d, pltpu.roll(cum, d, 1), 0.0)
        d *= 2
    total = jnp.broadcast_to(cum[:, CH - 1 : CH], (count, CH))
    carry = jnp.exp(total)
    reach = jnp.exp(total - cum)
    ecum = jnp.exp(cum)
    columns = jnp.transpose(
        jnp.concatenate([beta, cum, reach, jnp.zeros((CH - 3 * count, CH), F32)], axis=0)
    )
    row = iota((CH, CH), 0)
    col = iota((CH, CH), 1)
    eye = jnp.where(row == col, 1.0, 0.0)
    for s in range(seqs):
        for h in range(2):
            state = None
            for n in range(per_seq):
                m = s * per_seq + n
                r = 2 * m + h
                rows = slice(m * CH, (m + 1) * CH)
                lanes = slice(h * CH, (h + 1) * CH)
                k = kbuf[rows, lanes]
                v = vbuf[rows, lanes]
                gram = lax.dot_general(k, k, ABT, preferred_element_type=F32)
                gap = jnp.minimum(columns[:, count + r : count + r + 1] - cum[r : r + 1, :], 0.0)
                m_mat = jnp.where(row > col, columns[:, r : r + 1] * gram * jnp.exp(gap), 0.0)
                inv = inverse_of(m_mat)
                u = columns[:, 2 * count + r : 2 * count + r + 1] * inv * beta[r : r + 1, :]
                u2 = u * ecum[r : r + 1, :]
                uh, ul = split(u)
                u2h, u2l = split(u2)
                fresh = dot1(uh, v) + dot1(ul, v)
                pull = dot1(u2h, k) + dot1(u2l, k)
                wh, wl = split(jnp.concatenate([pull, fresh], axis=1))
                both = dot1(k, wh, ATB) + dot1(k, wl, ATB)
                dmap = both[:, :CH]
                c_row = carry[r : r + 1, :]
                if state is None:
                    state = jnp.concatenate([c_row * eye - dmap, both[:, CH:]], axis=1)
                else:
                    moved = dot3(dmap, state)
                    state = jnp.concatenate([c_row, c_row], axis=1) * state - moved
                    state = state + jnp.concatenate([jnp.zeros((CH, CH), F32), both[:, CH:]], axis=1)
            sbuf[2 * s + h, :CH, :] = state[:, :CH]
            sbuf[2 * s + h, CH:, :] = state[:, CH:]
    for k, o in enumerate((o0, o1, o2, o3)):
        o[...] = sbuf[lax.rem(here + k, 4)]


def ordered(refs, scr, here):
    for k, ref in enumerate(refs):
        scr[lax.rem(here + 4 - k, 4)] = ref[...]


def segments_kernel(r0, r1, r2, r3, o0, o1, o2, o3, scr, bscr):
    ordered((r0, r1, r2, r3), scr, lax.axis_index("sp_1"))
    there = lax.axis_index("sp_0")
    state = jnp.concatenate([scr[0, :CH, :], scr[0, CH:, :]], axis=1)
    for t in range(1, 4):
        state = dot3(scr[t, :CH, :], state)
        state = state + jnp.concatenate([jnp.zeros((CH, CH), F32), scr[t, CH:, :]], axis=1)
    bscr[...] = jnp.transpose(state[:, CH:])
    for k, o in enumerate((o0, o1, o2, o3)):
        q = lax.rem(there + k, 4)
        o[:CH, :] = state[:, :CH]
        o[CH:, :] = bscr[pl.ds(pl.multiple_of(q * 32, 32), 32), :]


def row_of(ref, s, h):
    two = ref[s].astype(F32)
    return jnp.sum(jnp.where(iota(two.shape, 0) == h, two, 0.0), axis=0, keepdims=True)


def columns_kernel(r0, r1, r2, r3, query_ref, key_ref, value_ref, gate_ref, out, scr, wide):
    part = lax.axis_index("sp_0")
    pair = lax.axis_index("sp_1")
    ordered((r0, r1, r2, r3), scr, part)
    f = scr[0, CH:, :]
    for g in range(1, 4):
        f = dot3(f, scr[g, :CH, :], ABT) + scr[g, CH:, :]
    s = pair // 2
    h = lax.rem(pair, 2)
    qn = unit_rows(row_of(query_ref, s, h))
    kn = unit_rows(row_of(key_ref, s, h))
    vn = row_of(value_ref, s, h)
    bn = 1.0 / (1.0 + jnp.exp(-jnp.full((1, CH), gate_ref[s, h], F32)))
    count = f.shape[0]
    mine = iota((count, CH), 1) == iota((count, CH), 0) + part * count
    vn_col = jnp.sum(jnp.where(mine, jnp.broadcast_to(vn, (count, CH)), 0.0), axis=1, keepdims=True)
    missing = vn_col - jnp.sum(f * kn, axis=1, keepdims=True)
    query_read = jnp.sum(f * qn, axis=1, keepdims=True)
    meet = jnp.sum(kn * qn, axis=1, keepdims=True)
    read = (query_read + (bn[:, :1] * meet) * missing) / math.sqrt(CH)
    wide[...] = jnp.zeros_like(wide)
    wide[pl.ds(pl.multiple_of(part * count, 32), count), :] = f + missing * (bn * kn)
    state = jnp.transpose(wide[...])
    read_row = jnp.sum(jnp.where(mine, jnp.broadcast_to(read, (count, CH)), 0.0), axis=0, keepdims=True)
    read_rows = jnp.broadcast_to(read_row, (8, CH))
    for p in range(out.shape[0]):
        out[p, :8, :] = state[8 * p : 8 * p + 8, :]
        out[p, 8:, :] = read_rows


def finish_kernel(r_ref, gain_ref, cache_ref, read_ref):
    for s in range(2):
        reads = []
        for h in range(2):
            j = 2 * s + h
            total = (r_ref[j] + r_ref[4 + j]) + (r_ref[8 + j] + r_ref[12 + j])
            cache_ref[s, h] = total[:8, :].astype(BF16)
            read = total[8:9, :]
            scale = lax.rsqrt(jnp.mean(read * read, axis=-1, keepdims=True) + 1e-06)
            reads.append(read * scale * gain_ref[...])
        read_ref[s] = jnp.concatenate(reads, axis=0).astype(BF16)


def vmem(count):
    return [pl.BlockSpec(memory_space=pltpu.VMEM) for _ in range(count)]


def spread(arrays, axis):
    out = [arrays[0]]
    for k in range(1, 4):
        out.append(lax.ppermute(arrays[k], axis, [(i, (i + k) % 4) for i in range(4)]))
    return out


def shards(
    tokens,
    key_matrix,
    value_matrix,
    gate_matrix,
    decay_matrix,
    gate_bias_offset,
    head_log_decay_rate,
    extra_log_decay,
    next_token_query,
    next_token_key,
    next_token_value,
    next_token_gate,
    readout_norm_gain,
):
    seqs, seg, width = tokens.shape
    cols = key_matrix.shape[1]
    tile = 256
    tiles = seqs * seg // tile
    count = seqs * seg // CH * 2
    smem = pl.BlockSpec(memory_space=pltpu.SMEM)
    hbm = pl.BlockSpec(memory_space=pl.ANY)
    maps = pl.pallas_call(
        maps_kernel,
        out_shape=[jax.ShapeDtypeStruct((2 * CH, CH), F32)] * 4,
        in_specs=[hbm, hbm, hbm, *vmem(2), smem, smem, *vmem(1)],
        out_specs=vmem(4),
        scratch_shapes=[
            pltpu.VMEM((tiles, tile, width), BF16),
            pltpu.VMEM((width, cols), BF16),
            pltpu.VMEM((width, cols), BF16),
            pltpu.VMEM((seqs * seg, cols), BF16),
            pltpu.VMEM((seqs * seg, cols), BF16),
            pltpu.VMEM((count, CH), F32),
            pltpu.VMEM((count, CH), F32),
            pltpu.VMEM((count, CH), F32),
            pltpu.VMEM((4, 2 * CH, CH), F32),
            pltpu.SemaphoreType.DMA((tiles + 2,)),
        ],
        compiler_params=pltpu.CompilerParams(vmem_limit_bytes=40 * 2**20),
        name="maps",
    )(
        tokens,
        key_matrix,
        value_matrix,
        gate_matrix.T,
        decay_matrix.T,
        gate_bias_offset,
        head_log_decay_rate,
        jnp.transpose(extra_log_decay, (0, 2, 1)),
    )
    pieces = pl.pallas_call(
        segments_kernel,
        out_shape=[jax.ShapeDtypeStruct((CH + 32, CH), F32)] * 4,
        in_specs=vmem(4),
        out_specs=vmem(4),
        scratch_shapes=[pltpu.VMEM((4, 2 * CH, CH), F32), pltpu.VMEM((CH, CH), F32)],
        name="segments",
    )(*spread(maps, "sp_1"))
    ranks = lax.axis_size(SP)
    rows = pl.pallas_call(
        columns_kernel,
        out_shape=jax.ShapeDtypeStruct((ranks, 16, CH), F32),
        in_specs=[*vmem(7), smem],
        out_specs=pl.BlockSpec(memory_space=pltpu.VMEM),
        scratch_shapes=[pltpu.VMEM((4, CH + 32, CH), F32), pltpu.VMEM((CH, CH), F32)],
        name="columns",
    )(*spread(pieces, "sp_0"), next_token_query, next_token_key, next_token_value, next_token_gate)
    got = lax.all_to_all(rows, SP, 0, 0, tiled=True)
    return pl.pallas_call(
        finish_kernel,
        out_shape=[
            jax.ShapeDtypeStruct((2, 2, 8, CH), BF16),
            jax.ShapeDtypeStruct((2, 2, CH), BF16),
        ],
        in_specs=vmem(2),
        out_specs=vmem(2),
        name="finish",
    )(got, readout_norm_gain.reshape(1, CH))


def solution(mesh):
    finer = Mesh(
        mesh.devices.reshape(mesh.shape["gr"], 4, 4, mesh.shape["tp"]), ("gr", "sp_0", "sp_1", "tp")
    )
    in_specs = (
        P("gr", SP, None),
        P(None, "tp"),
        P(None, "tp"),
        P(),
        P(),
        P(),
        P(),
        P("gr", SP, "tp"),
        P("gr", "tp", None),
        P("gr", "tp", None),
        P("gr", "tp", None),
        P("gr", "tp"),
        P(),
    )
    out_specs = (P("gr", "tp", SP, None), P("gr", "tp", None))
    return jax.shard_map(
        shards, mesh=finer, in_specs=in_specs, out_specs=out_specs, check_vma=False
    )
```

```python
import math

import jax
import jax.numpy as jnp
from jax import lax
from jax.experimental import pallas as pl
from jax.experimental.pallas import tpu as pltpu
from jax.sharding import Mesh
from jax.sharding import PartitionSpec as P

SP = ("sp_0", "sp_1")
CH = 128
F32 = jnp.float32
BF16 = jnp.bfloat16
AB = (((1,), (0,)), ((), ()))
ABT = (((1,), (1,)), ((), ()))
ATB = (((0,), (0,)), ((), ()))


def dot1(a, b, dims=AB):
    return lax.dot_general(a.astype(BF16), b.astype(BF16), dims, preferred_element_type=F32)


def split(a):
    hi = a.astype(BF16)
    return hi, (a - hi.astype(F32)).astype(BF16)


def dot3(a, b, dims=AB):
    ah, al = split(a)
    bh, bl = split(b)
    return dot1(ah, bh, dims) + (dot1(ah, bl, dims) + dot1(al, bh, dims))


def iota(shape, dim):
    return lax.broadcasted_iota(jnp.int32, shape, dim)


def unit_rows(a):
    return a * lax.rsqrt(jnp.sum(a * a, axis=-1, keepdims=True) + 1e-06)


def silu(a):
    return a * (1.0 / (1.0 + jnp.exp(-a)))


def inverses_of(m_mats):
    row = iota((CH, CH), 0)
    col = iota((CH, CH), 1)
    eye = jnp.where(row == col, 1.0, 0.0)
    near = row // 16 == col // 16
    p1s = [jnp.where(near, -m, 0.0) for m in m_mats]
    invs = [eye + p for p in p1s]
    pows = [p.astype(BF16) for p in p1s]
    pows = [dot1(p, p).astype(BF16) for p in pows]
    for last in (False, False, True):
        if last:
            adds = [dot1(p, i) for p, i in zip(pows, invs)]
        else:
            both = [dot1(p, jnp.concatenate([p, i.astype(BF16)], axis=1)) for p, i in zip(pows, invs)]
            adds = [x[:, CH:] for x in both]
            pows = [x[:, :CH].astype(BF16) for x in both]
        invs = [i + x for i, x in zip(invs, adds)]
    for b in (16, 32, 64):
        lower = [slice(s + b, s + 2 * b) for s in range(0, CH, 2 * b)]

        def gather(rows_of):
            return jnp.concatenate([rows_of(r) for r in lower], axis=0)

        m_rows = [
            gather(lambda r: jnp.where(col[r, :] // b == (r.start // b - 1), m[r, :], 0.0))
            for m in m_mats
        ]
        t_rows = [gather(lambda r: i[r, :]) for i in invs]
        ys = [dot1(m, i).astype(BF16) for m, i in zip(m_rows, invs)]
        spread_out = []
        for y in ys:
            pieces = []
            for g in range(len(lower)):
                pieces += [y[g * b : (g + 1) * b, :]] * 2
            spread_out.append(jnp.concatenate(pieces, axis=0))
        news = [t - dot1(t, y) for t, y in zip(t_rows, spread_out)]
        joined = []
        for i, new in zip(invs, news):
            pieces = []
            for g, r in enumerate(lower):
                pieces += [i[r.start - b : r.start, :], new[g * b : (g + 1) * b, :]]
            joined.append(jnp.concatenate(pieces, axis=0))
        invs = joined
    return invs


def maps_kernel(
    x_hbm, wk_hbm, wv_hbm, gate_hbm, decay_hbm, bias_hbm, rate_hbm, extra_hbm,
    o0, o1, o2, o3,
    xbuf, wkbuf, wvbuf, gatew, extra, bias_ref, rate_ref, kbuf, vbuf, rowbuf, state, sems,
):
    tiles, tile, width = xbuf.shape
    first_head = lax.axis_index("tp") * 2
    here = lax.axis_index("sp_1")
    per_tile = tile // CH
    per_seq = kbuf.shape[0] // (2 * CH)
    heads = gate_hbm.shape[0]

    def x_copy(t):
        half = tiles // 2
        rows = pl.ds(pl.multiple_of(lax.rem(t, half) * tile, tile), tile)
        return pltpu.make_async_copy(x_hbm.at[lax.div(t, half), rows], xbuf.at[t], sems.at[t])

    others = [
        pltpu.make_async_copy(src, dst, sems.at[tiles + i])
        for i, (src, dst) in enumerate(
            (
                (gate_hbm, gatew.at[pl.ds(0, heads)]),
                (decay_hbm, gatew.at[pl.ds(heads, heads)]),
                (wk_hbm, wkbuf),
                (wv_hbm, wvbuf),
                (bias_hbm, bias_ref),
                (rate_hbm, rate_ref),
                (extra_hbm, extra),
            )
        )
    ]
    for c in others[4:] + others[:3]:
        c.start()
    x_copy(0).start()
    others[3].start()
    for t in range(1, tiles):
        x_copy(t).start()
    for c in others[4:] + others[:3]:
        c.wait()
    pick = iota((heads, tile), 0)
    odd = iota((2, tile), 0) == 1
    bias = jnp.where(odd, bias_ref[first_head + 1], bias_ref[first_head])
    rate = jnp.exp(jnp.where(odd, rate_ref[first_head + 1], rate_ref[first_head]))
    row = iota((CH, CH), 0)
    col = iota((CH, CH), 1)
    eye = jnp.where(row == col, 1.0, 0.0)
    upto = jnp.where(row <= col, 1.0, 0.0).astype(BF16)

    def project(t, _):
        x_copy(t).wait()
        x = xbuf[t]
        gt = lax.dot_general(gatew[...], x, ABT, preferred_element_type=F32)
        picked = [
            jnp.sum(jnp.where(pick == first_head + h, part, 0.0), axis=0, keepdims=True)
            for part in (gt[:heads], gt[heads:])
            for h in range(2)
        ]
        beta = 1.0 / (1.0 + jnp.exp(-(jnp.concatenate(picked[:2], axis=0) + bias)))
        z = jnp.concatenate(picked[2:], axis=0)
        soft = jnp.maximum(z, 0.0) + jnp.log1p(jnp.exp(-jnp.abs(z)))
        for q in range(per_tile):
            m = t * per_tile + q
            lanes = slice(q * CH, (q + 1) * CH)
            step = extra[m] - rate[:, lanes] * soft[:, lanes]
            hi, rest = step.astype(BF16), step
            rest = rest - hi.astype(F32)
            mid = rest.astype(BF16)
            low = (rest - mid.astype(F32)).astype(BF16)
            cum = dot1(hi, upto) + (dot1(mid, upto) + dot1(low, upto))
            rowbuf[m, 0:2, :] = beta[:, lanes]
            rowbuf[m, 2:4, :] = cum

        @pl.when(t == 0)
        def _():
            others[3].wait()

        rows = pl.ds(pl.multiple_of(t * tile, tile), tile)
        kp = silu(lax.dot_general(x, wkbuf[...], AB, preferred_element_type=F32))
        for h in range(2):
            lanes = slice(h * CH, (h + 1) * CH)
            kbuf[rows, lanes] = unit_rows(kp[:, lanes]).astype(BF16)
        vp = silu(lax.dot_general(x, wvbuf[...], AB, preferred_element_type=F32))
        vbuf[rows, :] = vp.astype(BF16)
        return 0

    lax.fori_loop(0, tiles, project, 0)

    start = jnp.concatenate([eye, jnp.zeros((CH, CH), F32)], axis=1)
    for p in range(4):
        state[p] = start

    def advance(n, _):
        blocks = [rowbuf[n], rowbuf[per_seq + n]]
        beta = jnp.concatenate([b[0:2] for b in blocks], axis=0)
        cum = jnp.concatenate([b[2:4] for b in blocks], axis=0)
        total = jnp.broadcast_to(cum[:, CH - 1 : CH], (4, CH))
        carry = jnp.exp(total)
        reach = jnp.exp(total - cum)
        ecum = jnp.exp(cum)
        columns = jnp.transpose(
            jnp.concatenate([beta, cum, reach, jnp.zeros((CH - 12, CH), F32)], axis=0)
        )
        ks, vs, ms = [], [], []
        for p in range(4):
            s, h = divmod(p, 2)
            rows = pl.ds(pl.multiple_of((s * per_seq + n) * CH, CH), CH)
            lanes = slice(h * CH, (h + 1) * CH)
            ks.append(kbuf[rows, lanes])
            vs.append(vbuf[rows, lanes])
        grams = [lax.dot_general(k, k, ABT, preferred_element_type=F32) for k in ks]
        for p in range(4):
            gap = jnp.minimum(columns[:, 4 + p : 5 + p] - cum[p : p + 1, :], 0.0)
            ms.append(jnp.where(row > col, columns[:, p : p + 1] * grams[p] * jnp.exp(gap), 0.0))
        invs = inverses_of(ms)
        us = [columns[:, 8 + p : 9 + p] * invs[p] * beta[p : p + 1, :] for p in range(4)]
        pulls = [dot1(us[p] * ecum[p : p + 1, :], ks[p]).astype(BF16) for p in range(4)]
        freshs = [dot1(us[p], vs[p]).astype(BF16) for p in range(4)]
        boths = [
            dot1(k, jnp.concatenate([pull, fresh], axis=1), ATB)
            for k, pull, fresh in zip(ks, pulls, freshs)
        ]
        for p in range(4):
            before = state[p]
            moved = dot1(boths[p][:, :CH], before)
            c_row = carry[p : p + 1, :]
            state[p, :, :CH] = c_row * before[:, :CH] - moved[:, :CH]
            state[p, :, CH:] = c_row * before[:, CH:] - moved[:, CH:] + boths[p][:, CH:]
        return 0

    lax.fori_loop(0, per_seq, advance, 0)
    for k, o in enumerate((o0, o1, o2, o3)):
        p = lax.rem(here + k, 4)
        o[:CH, :] = state[p, :, :CH]
        o[CH:, :] = state[p, :, CH:]


def ordered(refs, scr, here):
    for k, ref in enumerate(refs):
        scr[lax.rem(here + 4 - k, 4)] = ref[...]


def segments_kernel(r0, r1, r2, r3, o0, o1, o2, o3, scr, bscr):
    ordered((r0, r1, r2, r3), scr, lax.axis_index("sp_1"))
    there = lax.axis_index("sp_0")
    state = jnp.concatenate([scr[0, :CH, :], scr[0, CH:, :]], axis=1)
    for t in range(1, 4):
        state = dot3(scr[t, :CH, :], state)
        state = state + jnp.concatenate([jnp.zeros((CH, CH), F32), scr[t, CH:, :]], axis=1)
    bscr[...] = jnp.transpose(state[:, CH:])
    for k, o in enumerate((o0, o1, o2, o3)):
        q = lax.rem(there + k, 4)
        o[:CH, :] = state[:, :CH]
        o[CH:, :] = bscr[pl.ds(pl.multiple_of(q * 32, 32), 32), :]


def row_of(ref, s, h):
    two = ref[s].astype(F32)
    return jnp.sum(jnp.where(iota(two.shape, 0) == h, two, 0.0), axis=0, keepdims=True)


def columns_kernel(r0, r1, r2, r3, query_ref, key_ref, value_ref, gate_ref, out, scr, wide):
    part = lax.axis_index("sp_0")
    pair = lax.axis_index("sp_1")
    ordered((r0, r1, r2, r3), scr, part)
    f = scr[0, CH:, :]
    for g in range(1, 4):
        f = dot3(f, scr[g, :CH, :], ABT) + scr[g, CH:, :]
    s = pair // 2
    h = lax.rem(pair, 2)
    qn = unit_rows(row_of(query_ref, s, h))
    kn = unit_rows(row_of(key_ref, s, h))
    vn = row_of(value_ref, s, h)
    bn = 1.0 / (1.0 + jnp.exp(-jnp.full((1, CH), gate_ref[s, h], F32)))
    count = f.shape[0]
    mine = iota((count, CH), 1) == iota((count, CH), 0) + part * count
    vn_col = jnp.sum(jnp.where(mine, jnp.broadcast_to(vn, (count, CH)), 0.0), axis=1, keepdims=True)
    missing = vn_col - jnp.sum(f * kn, axis=1, keepdims=True)
    query_read = jnp.sum(f * qn, axis=1, keepdims=True)
    meet = jnp.sum(kn * qn, axis=1, keepdims=True)
    read = (query_read + (bn[:, :1] * meet) * missing) / math.sqrt(CH)
    wide[...] = jnp.zeros_like(wide)
    wide[pl.ds(pl.multiple_of(part * count, 32), count), :] = f + missing * (bn * kn)
    state = jnp.transpose(wide[...])
    read_row = jnp.sum(jnp.where(mine, jnp.broadcast_to(read, (count, CH)), 0.0), axis=0, keepdims=True)
    read_rows = jnp.broadcast_to(read_row, (8, CH))
    for p in range(out.shape[0]):
        out[p, :8, :] = state[8 * p : 8 * p + 8, :]
        out[p, 8:, :] = read_rows


def finish_kernel(r_ref, gain_ref, cache_ref, read_ref):
    for s in range(2):
        reads = []
        for h in range(2):
            j = 2 * s + h
            total = (r_ref[j] + r_ref[4 + j]) + (r_ref[8 + j] + r_ref[12 + j])
            cache_ref[s, h] = total[:8, :].astype(BF16)
            read = total[8:9, :]
            scale = lax.rsqrt(jnp.mean(read * read, axis=-1, keepdims=True) + 1e-06)
            reads.append(read * scale * gain_ref[...])
        read_ref[s] = jnp.concatenate(reads, axis=0).astype(BF16)


def vmem(count):
    return [pl.BlockSpec(memory_space=pltpu.VMEM) for _ in range(count)]


def spread(arrays, axis):
    out = [arrays[0]]
    for k in range(1, 4):
        out.append(lax.ppermute(arrays[k], axis, [(i, (i + k) % 4) for i in range(4)]))
    return out


def shards(
    tokens,
    key_matrix,
    value_matrix,
    gate_matrix,
    decay_matrix,
    gate_bias_offset,
    head_log_decay_rate,
    extra_log_decay,
    next_token_query,
    next_token_key,
    next_token_value,
    next_token_gate,
    readout_norm_gain,
):
    seqs, seg, width = tokens.shape
    cols = key_matrix.shape[1]
    tile = 256
    tiles = seqs * seg // tile
    chunks = seqs * seg // CH
    extra = jnp.transpose(extra_log_decay.reshape(chunks, CH, 2), (0, 2, 1))
    hbm = pl.BlockSpec(memory_space=pltpu.HBM)
    smem = pl.BlockSpec(memory_space=pltpu.SMEM)
    maps = pl.pallas_call(
        maps_kernel,
        out_shape=[jax.ShapeDtypeStruct((2 * CH, CH), F32)] * 4,
        in_specs=[hbm] * 8,
        out_specs=vmem(4),
        scratch_shapes=[
            pltpu.VMEM((tiles, tile, width), BF16),
            pltpu.VMEM((width, cols), BF16),
            pltpu.VMEM((width, cols), BF16),
            pltpu.VMEM((2 * gate_matrix.shape[1], width), BF16),
            pltpu.VMEM((chunks, 2, CH), F32),
            pltpu.SMEM(gate_bias_offset.shape, F32),
            pltpu.SMEM(head_log_decay_rate.shape, F32),
            pltpu.VMEM((seqs * seg, cols), BF16),
            pltpu.VMEM((seqs * seg, cols), BF16),
            pltpu.VMEM((chunks, 8, CH), F32),
            pltpu.VMEM((4, CH, 2 * CH), F32),
            pltpu.SemaphoreType.DMA((tiles + 7,)),
        ],
        compiler_params=pltpu.CompilerParams(vmem_limit_bytes=24 * 2**20),
        name="maps",
    )(
        *(
            pltpu.with_memory_space_constraint(a, pltpu.HBM)
            for a in (
                tokens,
                key_matrix,
                value_matrix,
                gate_matrix.T,
                decay_matrix.T,
                gate_bias_offset,
                head_log_decay_rate,
                extra,
            )
        )
    )
    small = pltpu.CompilerParams(vmem_limit_bytes=8 * 2**20)
    pieces = pl.pallas_call(
        segments_kernel,
        out_shape=[jax.ShapeDtypeStruct((CH + 32, CH), F32)] * 4,
        in_specs=vmem(4),
        out_specs=vmem(4),
        scratch_shapes=[pltpu.VMEM((4, 2 * CH, CH), F32), pltpu.VMEM((CH, CH), F32)],
        compiler_params=small,
        name="segments",
    )(*spread(maps, "sp_1"))
    ranks = lax.axis_size(SP)
    rows = pl.pallas_call(
        columns_kernel,
        out_shape=jax.ShapeDtypeStruct((ranks, 16, CH), F32),
        in_specs=[*vmem(7), smem],
        out_specs=pl.BlockSpec(memory_space=pltpu.VMEM),
        scratch_shapes=[pltpu.VMEM((4, CH + 32, CH), F32), pltpu.VMEM((CH, CH), F32)],
        compiler_params=small,
        name="columns",
    )(*spread(pieces, "sp_0"), next_token_query, next_token_key, next_token_value, next_token_gate)
    got = lax.all_to_all(rows, SP, 0, 0, tiled=True)
    return pl.pallas_call(
        finish_kernel,
        out_shape=[
            jax.ShapeDtypeStruct((2, 2, 8, CH), BF16),
            jax.ShapeDtypeStruct((2, 2, CH), BF16),
        ],
        in_specs=vmem(2),
        out_specs=vmem(2),
        compiler_params=small,
        name="finish",
    )(got, readout_norm_gain.reshape(1, CH))


def solution(mesh):
    finer = Mesh(
        mesh.devices.reshape(mesh.shape["gr"], 4, 4, mesh.shape["tp"]), ("gr", "sp_0", "sp_1", "tp")
    )
    in_specs = (
        P("gr", SP, None),
        P(None, "tp"),
        P(None, "tp"),
        P(),
        P(),
        P(),
        P(),
        P("gr", SP, "tp"),
        P("gr", "tp", None),
        P("gr", "tp", None),
        P("gr", "tp", None),
        P("gr", "tp"),
        P(),
    )
    out_specs = (P("gr", "tp", SP, None), P("gr", "tp", None))
    return jax.shard_map(
        shards, mesh=finer, in_specs=in_specs, out_specs=out_specs, check_vma=False
    )
```

```python
import math

import jax
import jax.numpy as jnp
from jax import lax
from jax.experimental import pallas as pl
from jax.experimental.pallas import tpu as pltpu
from jax.sharding import Mesh
from jax.sharding import PartitionSpec as P

SP = ("sp_0", "sp_1")
CH = 128
F32 = jnp.float32
BF16 = jnp.bfloat16
AB = (((1,), (0,)), ((), ()))
ABT = (((1,), (1,)), ((), ()))
ATB = (((0,), (0,)), ((), ()))


def dot1(a, b, dims=AB):
    return lax.dot_general(a.astype(BF16), b.astype(BF16), dims, preferred_element_type=F32)


def split(a):
    hi = a.astype(BF16)
    return hi, (a - hi.astype(F32)).astype(BF16)


def dot3(a, b, dims=AB):
    ah, al = split(a)
    bh, bl = split(b)
    return dot1(ah, bh, dims) + (dot1(ah, bl, dims) + dot1(al, bh, dims))


def iota(shape, dim):
    return lax.broadcasted_iota(jnp.int32, shape, dim)


def unit_rows(a):
    return a * lax.rsqrt(jnp.sum(a * a, axis=-1, keepdims=True) + 1e-06)


def silu(a):
    return a * (1.0 / (1.0 + jnp.exp(-a)))


def inverses_of(m_mats):
    row = iota((CH, CH), 0)
    col = iota((CH, CH), 1)
    eye = jnp.where(row == col, 1.0, 0.0)
    near = row // 16 == col // 16
    p1s = [jnp.where(near, -m, 0.0) for m in m_mats]
    invs = [eye + p for p in p1s]
    pows = [p.astype(BF16) for p in p1s]
    pows = [dot1(p, p).astype(BF16) for p in pows]
    for last in (False, False, True):
        if last:
            adds = [dot1(p, i) for p, i in zip(pows, invs)]
        else:
            both = [dot1(p, jnp.concatenate([p, i.astype(BF16)], axis=1)) for p, i in zip(pows, invs)]
            adds = [x[:, CH:] for x in both]
            pows = [x[:, :CH].astype(BF16) for x in both]
        invs = [i + x for i, x in zip(invs, adds)]
    for b in (16, 32, 64):
        lower = [slice(s + b, s + 2 * b) for s in range(0, CH, 2 * b)]

        def gather(rows_of):
            return jnp.concatenate([rows_of(r) for r in lower], axis=0)

        m_rows = [
            gather(lambda r: jnp.where(col[r, :] // b == (r.start // b - 1), m[r, :], 0.0))
            for m in m_mats
        ]
        t_rows = [gather(lambda r: i[r, :]) for i in invs]
        ys = [dot1(m, i).astype(BF16) for m, i in zip(m_rows, invs)]
        spread_out = []
        for y in ys:
            pieces = []
            for g in range(len(lower)):
                pieces += [jnp.zeros((b, CH), BF16), y[g * b : (g + 1) * b, :]]
            spread_out.append(jnp.concatenate(pieces, axis=0))
        news = [t - dot1(t, y) for t, y in zip(t_rows, spread_out)]
        joined = []
        for i, new in zip(invs, news):
            pieces = []
            for g, r in enumerate(lower):
                pieces += [i[r.start - b : r.start, :], new[g * b : (g + 1) * b, :]]
            joined.append(jnp.concatenate(pieces, axis=0))
        invs = joined
    return invs


def maps_kernel(
    x_hbm, wk_hbm, wv_hbm, gate_hbm, decay_hbm, bias_hbm, rate_hbm, extra_hbm,
    o0, o1, o2, o3,
    xbuf, wkbuf, wvbuf, gatew, extra, bias_ref, rate_ref, kbuf, vbuf, state, sems,
):
    tiles, tile, width = xbuf.shape
    first_head = lax.axis_index("tp") * 2
    here = lax.axis_index("sp_1")
    per_seq = kbuf.shape[0] // (2 * CH)
    heads = gate_hbm.shape[0]

    def x_copy(t):
        s, part = divmod(t, tiles // 2)
        rows = pl.ds(part * tile, tile)
        return pltpu.make_async_copy(x_hbm.at[s, rows], xbuf.at[t], sems.at[t])

    others = [
        pltpu.make_async_copy(src, dst, sems.at[tiles + i])
        for i, (src, dst) in enumerate(
            (
                (gate_hbm, gatew.at[pl.ds(0, heads)]),
                (decay_hbm, gatew.at[pl.ds(heads, heads)]),
                (wk_hbm, wkbuf),
                (wv_hbm, wvbuf),
                (bias_hbm, bias_ref),
                (rate_hbm, rate_ref),
                (extra_hbm, extra),
            )
        )
    ]
    for c in others[4:] + others[:3]:
        c.start()
    x_copy(0).start()
    others[3].start()
    for t in range(1, tiles):
        x_copy(t).start()
    for c in others[4:] + others[:3]:
        c.wait()
    pick = iota((heads, tile), 0)
    odd = iota((2, tile), 0) == 1
    bias = jnp.where(odd, bias_ref[first_head + 1], bias_ref[first_head])
    rate = jnp.exp(jnp.where(odd, rate_ref[first_head + 1], rate_ref[first_head]))
    row = iota((CH, CH), 0)
    col = iota((CH, CH), 1)
    eye = jnp.where(row == col, 1.0, 0.0)
    upto = jnp.where(row <= col, 1.0, 0.0).astype(BF16)

    def halves(t, weights, dims, count):
        size = tile // count
        return [
            lax.dot_general(
                xbuf[t, i * size : (i + 1) * size], weights[...], dims, preferred_element_type=F32
            )
            for i in range(count)
        ]

    def scalars(t, gt):
        picked = [
            jnp.sum(jnp.where(pick == first_head + h, part, 0.0), axis=0, keepdims=True)
            for part in (gt[:heads], gt[heads:])
            for h in range(2)
        ]
        z = jnp.concatenate(picked[2:], axis=0)
        soft = jnp.maximum(z, 0.0) + jnp.log1p(jnp.exp(-jnp.abs(z)))
        gate = jnp.concatenate(picked[:2], axis=0) + bias
        steps, gates = [], []
        for n in range(per_seq):
            lanes = slice(n * CH, (n + 1) * CH)
            steps.append(extra[t * per_seq + n] - rate[:, lanes] * soft[:, lanes])
            gates.append(gate[:, lanes])
        step = jnp.concatenate(steps, axis=0)
        beta = 1.0 / (1.0 + jnp.exp(-jnp.concatenate(gates, axis=0)))
        hi = step.astype(BF16)
        rest = step - hi.astype(F32)
        mid = rest.astype(BF16)
        low = (rest - mid.astype(F32)).astype(BF16)
        cum = dot1(hi, upto) + (dot1(mid, upto) + dot1(low, upto))
        count = cum.shape[0]
        total = jnp.broadcast_to(cum[:, CH - 1 : CH], (count, CH))
        columns = jnp.transpose(
            jnp.concatenate(
                [cum + jnp.log(beta), jnp.exp(total - cum), jnp.zeros((CH - 2 * count, CH), F32)], axis=0
            )
        )
        return beta, cum, jnp.exp(total), jnp.exp(cum), columns

    def weighted(t, kp, rows):
        kp = silu(kp)
        for h in range(2):
            lanes = slice(h * CH, (h + 1) * CH)
            kbuf[rows, lanes] = unit_rows(kp[:, lanes]).astype(BF16)

    def matrices(t, cum, columns):
        ms = []
        for n in range(per_seq):
            for h in range(2):
                k = part(kbuf, t, n, h)
                gram = lax.dot_general(k, k, ABT, preferred_element_type=F32)
                r = 2 * n + h
                ms.append(jnp.where(row > col, gram * jnp.exp(columns[:, r : r + 1] - cum[r : r + 1, :]), 0.0))
        return ms

    def part(buf, s, n, h):
        start = (s * per_seq + n) * CH
        return buf[start : start + CH, h * CH : (h + 1) * CH]

    rows_of = []
    ms = []
    for t in range(tiles):
        x_copy(t).wait()
        gt = jnp.concatenate([jnp.transpose(g) for g in halves(t, gatew, ABT, 2)], axis=1)
        count = 2 if True or (True and t == tiles - 1) else 1
        size = tile // count
        kps = halves(t, wkbuf, AB, count)
        if t == 0:
            others[3].wait()
        vps = halves(t, wvbuf, AB, count)
        rows_of.append(scalars(t, gt))
        for i in range(count):
            weighted(t, kps[i], slice(t * tile + i * size, t * tile + (i + 1) * size))
        ms += matrices(t, rows_of[t][1], rows_of[t][4])
        for i in range(count):
            vbuf[t * tile + i * size : t * tile + (i + 1) * size, :] = silu(vps[i]).astype(BF16)

    items = [(s, n, h) for s in range(2) for n in range(per_seq) for h in range(2)]
    invs = inverses_of(ms)
    us = []
    for (s, n, h), inv in zip(items, invs):
        beta, _, _, _, columns = rows_of[s]
        r = 2 * n + h
        us.append(columns[:, 8 + r : 9 + r] * inv * beta[r : r + 1, :])
    pulls = [
        dot1(u * rows_of[s][3][2 * n + h : 2 * n + h + 1, :], part(kbuf, s, n, h)).astype(BF16)
        for (s, n, h), u in zip(items, us)
    ]
    freshs = [dot1(u, part(vbuf, s, n, h)).astype(BF16) for (s, n, h), u in zip(items, us)]
    boths = {
        (s, n, h): dot1(part(kbuf, s, n, h), jnp.concatenate([pull, fresh], axis=1), ATB)
        for (s, n, h), pull, fresh in zip(items, pulls, freshs)
    }
    for n in range(per_seq):
        for p in range(4):
            s, h = divmod(p, 2)
            both = boths[s, n, h]
            c_row = rows_of[s][2][2 * n + h : 2 * n + h + 1, :]
            if n == 0:
                state[p, :, :CH] = c_row * eye - both[:, :CH]
                state[p, :, CH:] = both[:, CH:]
                continue
            before = state[p]
            moved = dot1(both[:, :CH], before)
            state[p, :, :CH] = c_row * before[:, :CH] - moved[:, :CH]
            state[p, :, CH:] = c_row * before[:, CH:] - moved[:, CH:] + both[:, CH:]

    for k, o in enumerate((o0, o1, o2, o3)):
        p = lax.rem(here + k, 4)
        o[:CH, :] = state[p, :, :CH]
        o[CH:, :] = state[p, :, CH:]


def ordered(refs, scr, here):
    for k, ref in enumerate(refs):
        scr[lax.rem(here + 4 - k, 4)] = ref[...]


def segments_kernel(r0, r1, r2, r3, o0, o1, o2, o3, scr, bscr):
    ordered((r0, r1, r2, r3), scr, lax.axis_index("sp_1"))
    there = lax.axis_index("sp_0")
    state = jnp.concatenate([scr[0, :CH, :], scr[0, CH:, :]], axis=1)
    for t in range(1, 4):
        state = dot3(scr[t, :CH, :], state)
        state = state + jnp.concatenate([jnp.zeros((CH, CH), F32), scr[t, CH:, :]], axis=1)
    bscr[...] = jnp.transpose(state[:, CH:])
    for k, o in enumerate((o0, o1, o2, o3)):
        q = lax.rem(there + k, 4)
        o[:CH, :] = state[:, :CH]
        o[CH:, :] = bscr[pl.ds(pl.multiple_of(q * 32, 32), 32), :]


def row_of(ref, s, h):
    two = ref[s].astype(F32)
    return jnp.sum(jnp.where(iota(two.shape, 0) == h, two, 0.0), axis=0, keepdims=True)


def columns_kernel(r0, r1, r2, r3, query_ref, key_ref, value_ref, gate_ref, out, scr, wide):
    part = lax.axis_index("sp_0")
    pair = lax.axis_index("sp_1")
    ordered((r0, r1, r2, r3), scr, part)
    f = scr[0, CH:, :]
    for g in range(1, 4):
        f = dot3(f, scr[g, :CH, :], ABT) + scr[g, CH:, :]
    s = pair // 2
    h = lax.rem(pair, 2)
    qn = unit_rows(row_of(query_ref, s, h))
    kn = unit_rows(row_of(key_ref, s, h))
    vn = row_of(value_ref, s, h)
    bn = 1.0 / (1.0 + jnp.exp(-jnp.full((1, CH), gate_ref[s, h], F32)))
    count = f.shape[0]
    mine = iota((count, CH), 1) == iota((count, CH), 0) + part * count
    vn_col = jnp.sum(jnp.where(mine, jnp.broadcast_to(vn, (count, CH)), 0.0), axis=1, keepdims=True)
    missing = vn_col - jnp.sum(f * kn, axis=1, keepdims=True)
    query_read = jnp.sum(f * qn, axis=1, keepdims=True)
    meet = jnp.sum(kn * qn, axis=1, keepdims=True)
    read = (query_read + (bn[:, :1] * meet) * missing) / math.sqrt(CH)
    wide[...] = jnp.zeros_like(wide)
    wide[pl.ds(pl.multiple_of(part * count, 32), count), :] = f + missing * (bn * kn)
    state = jnp.transpose(wide[...])
    read_row = jnp.sum(jnp.where(mine, jnp.broadcast_to(read, (count, CH)), 0.0), axis=0, keepdims=True)
    read_rows = jnp.broadcast_to(read_row, (8, CH))
    for p in range(out.shape[0]):
        out[p, :8, :] = state[8 * p : 8 * p + 8, :]
        out[p, 8:, :] = read_rows


def finish_kernel(r_ref, gain_ref, cache_ref, read_ref):
    for s in range(2):
        reads = []
        for h in range(2):
            j = 2 * s + h
            total = (r_ref[j] + r_ref[4 + j]) + (r_ref[8 + j] + r_ref[12 + j])
            cache_ref[s, h] = total[:8, :].astype(BF16)
            read = total[8:9, :]
            scale = lax.rsqrt(jnp.mean(read * read, axis=-1, keepdims=True) + 1e-06)
            reads.append(read * scale * gain_ref[...])
        read_ref[s] = jnp.concatenate(reads, axis=0).astype(BF16)


def vmem(count):
    return [pl.BlockSpec(memory_space=pltpu.VMEM) for _ in range(count)]


def spread(arrays, axis):
    out = [arrays[0]]
    for k in range(1, 4):
        out.append(lax.ppermute(arrays[k], axis, [(i, (i + k) % 4) for i in range(4)]))
    return out


def shards(
    tokens,
    key_matrix,
    value_matrix,
    gate_matrix,
    decay_matrix,
    gate_bias_offset,
    head_log_decay_rate,
    extra_log_decay,
    next_token_query,
    next_token_key,
    next_token_value,
    next_token_gate,
    readout_norm_gain,
):
    seqs, seg, width = tokens.shape
    cols = key_matrix.shape[1]
    tile = seg
    tiles = seqs * seg // tile
    chunks = seqs * seg // CH
    extra = jnp.transpose(extra_log_decay.reshape(chunks, CH, 2), (0, 2, 1))
    hbm = pl.BlockSpec(memory_space=pltpu.HBM)
    smem = pl.BlockSpec(memory_space=pltpu.SMEM)
    maps = pl.pallas_call(
        maps_kernel,
        out_shape=[jax.ShapeDtypeStruct((2 * CH, CH), F32)] * 4,
        in_specs=[hbm] * 8,
        out_specs=vmem(4),
        scratch_shapes=[
            pltpu.VMEM((tiles, tile, width), BF16),
            pltpu.VMEM((width, cols), BF16),
            pltpu.VMEM((width, cols), BF16),
            pltpu.VMEM((2 * gate_matrix.shape[1], width), BF16),
            pltpu.VMEM((chunks, 2, CH), F32),
            pltpu.SMEM(gate_bias_offset.shape, F32),
            pltpu.SMEM(head_log_decay_rate.shape, F32),
            pltpu.VMEM((seqs * seg, cols), BF16),
            pltpu.VMEM((seqs * seg, cols), BF16),
            pltpu.VMEM((4, CH, 2 * CH), F32),
            pltpu.SemaphoreType.DMA((tiles + 7,)),
        ],
        compiler_params=pltpu.CompilerParams(vmem_limit_bytes=24 * 2**20),
        name="maps",
    )(
        *(
            pltpu.with_memory_space_constraint(a, pltpu.HBM)
            for a in (
                tokens,
                key_matrix,
                value_matrix,
                gate_matrix.T,
                decay_matrix.T,
                gate_bias_offset,
                head_log_decay_rate,
                extra,
            )
        )
    )
    small = pltpu.CompilerParams(vmem_limit_bytes=8 * 2**20)
    pieces = pl.pallas_call(
        segments_kernel,
        out_shape=[jax.ShapeDtypeStruct((CH + 32, CH), F32)] * 4,
        in_specs=vmem(4),
        out_specs=vmem(4),
        scratch_shapes=[pltpu.VMEM((4, 2 * CH, CH), F32), pltpu.VMEM((CH, CH), F32)],
        compiler_params=small,
        name="segments",
    )(*spread(maps, "sp_1"))
    ranks = lax.axis_size(SP)
    rows = pl.pallas_call(
        columns_kernel,
        out_shape=jax.ShapeDtypeStruct((ranks, 16, CH), F32),
        in_specs=[*vmem(7), smem],
        out_specs=pl.BlockSpec(memory_space=pltpu.VMEM),
        scratch_shapes=[pltpu.VMEM((4, CH + 32, CH), F32), pltpu.VMEM((CH, CH), F32)],
        compiler_params=small,
        name="columns",
    )(*spread(pieces, "sp_0"), next_token_query, next_token_key, next_token_value, next_token_gate)
    got = lax.all_to_all(rows, SP, 0, 0, tiled=True)
    return pl.pallas_call(
        finish_kernel,
        out_shape=[
            jax.ShapeDtypeStruct((2, 2, 8, CH), BF16),
            jax.ShapeDtypeStruct((2, 2, CH), BF16),
        ],
        in_specs=vmem(2),
        out_specs=vmem(2),
        compiler_params=small,
        name="finish",
    )(got, readout_norm_gain.reshape(1, CH))


def solution(mesh):
    finer = Mesh(
        mesh.devices.reshape(mesh.shape["gr"], 4, 4, mesh.shape["tp"]), ("gr", "sp_0", "sp_1", "tp")
    )
    in_specs = (
        P("gr", SP, None),
        P(None, "tp"),
        P(None, "tp"),
        P(),
        P(),
        P(),
        P(),
        P("gr", SP, "tp"),
        P("gr", "tp", None),
        P("gr", "tp", None),
        P("gr", "tp", None),
        P("gr", "tp"),
        P(),
    )
    out_specs = (P("gr", "tp", SP, None), P("gr", "tp", None))
    return jax.shard_map(
        shards, mesh=finer, in_specs=in_specs, out_specs=out_specs, check_vma=False
    )
```

```python
import math

import jax
import jax.numpy as jnp
from jax import lax
from jax.experimental import pallas as pl
from jax.experimental.pallas import tpu as pltpu
from jax.sharding import Mesh
from jax.sharding import PartitionSpec as P

SP = ("sp_0", "sp_1")
CH = 128
ROWS = 32
SHIFTS = (0, 2, 3, 1)
F32 = jnp.float32
BF16 = jnp.bfloat16
AB = (((1,), (0,)), ((), ()))
ABT = (((1,), (1,)), ((), ()))
ATB = (((0,), (0,)), ((), ()))


def dot1(a, b, dims=AB):
    return lax.dot_general(a.astype(BF16), b.astype(BF16), dims, preferred_element_type=F32)


def split(a):
    hi = a.astype(BF16)
    return hi, (a - hi.astype(F32)).astype(BF16)


def dot3(a, b, dims=AB):
    ah, al = split(a)
    bh, bl = split(b)
    return dot1(ah, bh, dims) + (dot1(ah, bl, dims) + dot1(al, bh, dims))


def iota(shape, dim):
    return lax.broadcasted_iota(jnp.int32, shape, dim)


def unit_rows(a):
    return a * lax.rsqrt(jnp.sum(a * a, axis=-1, keepdims=True) + 1e-06)


def silu(a):
    return a * (1.0 / (1.0 + jnp.exp(-a)))


def inverses_of(m_mats):
    row = iota((CH, CH), 0)
    col = iota((CH, CH), 1)
    eye = jnp.where(row == col, 1.0, 0.0)
    near = row // 16 == col // 16
    p1s = [jnp.where(near, -m, 0.0) for m in m_mats]
    invs = [eye + p for p in p1s]
    pows = [p.astype(BF16) for p in p1s]
    pows = [dot1(p, p).astype(BF16) for p in pows]
    for last in (False, False, True):
        if last:
            adds = [dot1(p, i) for p, i in zip(pows, invs)]
        else:
            both = [dot1(p, jnp.concatenate([p, i.astype(BF16)], axis=1)) for p, i in zip(pows, invs)]
            adds = [x[:, CH:] for x in both]
            pows = [x[:, :CH].astype(BF16) for x in both]
        invs = [i + x for i, x in zip(invs, adds)]
    for b in (16, 32, 64):
        lower = [slice(s + b, s + 2 * b) for s in range(0, CH, 2 * b)]

        def gather(rows_of):
            return jnp.concatenate([rows_of(r) for r in lower], axis=0)

        m_rows = [
            gather(lambda r: jnp.where(col[r, :] // b == (r.start // b - 1), m[r, :], 0.0))
            for m in m_mats
        ]
        t_rows = [gather(lambda r: i[r, :]) for i in invs]
        ys = [dot1(m, i).astype(BF16) for m, i in zip(m_rows, invs)]
        spread_out = []
        for y in ys:
            pieces = []
            for g in range(len(lower)):
                pieces += [jnp.zeros((b, CH), BF16), y[g * b : (g + 1) * b, :]]
            spread_out.append(jnp.concatenate(pieces, axis=0))
        news = [t - dot1(t, y) for t, y in zip(t_rows, spread_out)]
        joined = []
        for i, new in zip(invs, news):
            pieces = []
            for g, r in enumerate(lower):
                pieces += [i[r.start - b : r.start, :], new[g * b : (g + 1) * b, :]]
            joined.append(jnp.concatenate(pieces, axis=0))
        invs = joined
    return invs


def joined(first, second, eye):
    c1, d1, b1 = first
    c2, d2, b2 = second
    moved = dot1(d2, jnp.concatenate([c1 * eye - d1, b1], axis=1))
    return c1 * c2, c2 * d1 + moved[:, :CH], c2 * b1 - moved[:, CH:] + b2


def maps_kernel(
    x_hbm, wk_hbm, wv_hbm, gate_hbm, decay_hbm, bias_hbm, rate_hbm, extra_hbm,
    o0, o1, o2, o3,
    xbuf, wkbuf, wvbuf, gatew, extra, bias_ref, rate_ref, kbuf, vbuf, state, sems,
):
    tiles, tile, width = xbuf.shape
    first_head = lax.axis_index("tp") * 2
    here = lax.axis_index("sp_1")
    per_seq = kbuf.shape[0] // (2 * CH)
    heads = gate_hbm.shape[0]

    def x_copy(t):
        s, part = divmod(t, tiles // 2)
        rows = pl.ds(part * tile, tile)
        return pltpu.make_async_copy(x_hbm.at[s, rows], xbuf.at[t], sems.at[t])

    others = [
        pltpu.make_async_copy(src, dst, sems.at[tiles + i])
        for i, (src, dst) in enumerate(
            (
                (gate_hbm, gatew.at[pl.ds(0, heads)]),
                (decay_hbm, gatew.at[pl.ds(heads, heads)]),
                (wk_hbm, wkbuf),
                (wv_hbm, wvbuf),
                (bias_hbm, bias_ref),
                (rate_hbm, rate_ref),
                (extra_hbm, extra),
            )
        )
    ]
    for c in others[4:] + others[:3]:
        c.start()
    x_copy(0).start()
    others[3].start()
    for t in range(1, tiles):
        x_copy(t).start()
    for c in others[4:] + others[:3]:
        c.wait()
    pick = iota((heads, tile), 0)
    odd = iota((2, tile), 0) == 1
    bias = jnp.where(odd, bias_ref[first_head + 1], bias_ref[first_head])
    rate = jnp.exp(jnp.where(odd, rate_ref[first_head + 1], rate_ref[first_head]))
    row = iota((CH, CH), 0)
    col = iota((CH, CH), 1)
    eye = jnp.where(row == col, 1.0, 0.0)
    upto = jnp.where(row <= col, 1.0, 0.0).astype(BF16)

    def halves(t, weights, dims, count):
        size = tile // count
        return [
            lax.dot_general(
                xbuf[t, i * size : (i + 1) * size], weights[...], dims, preferred_element_type=F32
            )
            for i in range(count)
        ]

    def scalars(t, gt):
        picked = [
            jnp.sum(jnp.where(pick == first_head + h, part, 0.0), axis=0, keepdims=True)
            for part in (gt[:heads], gt[heads:])
            for h in range(2)
        ]
        z = jnp.concatenate(picked[2:], axis=0)
        soft = jnp.maximum(z, 0.0) + jnp.log1p(jnp.exp(-jnp.abs(z)))
        gate = jnp.concatenate(picked[:2], axis=0) + bias
        steps, gates = [], []
        for n in range(per_seq):
            lanes = slice(n * CH, (n + 1) * CH)
            steps.append(extra[t * per_seq + n] - rate[:, lanes] * soft[:, lanes])
            gates.append(gate[:, lanes])
        step = jnp.concatenate(steps, axis=0)
        beta = 1.0 / (1.0 + jnp.exp(-jnp.concatenate(gates, axis=0)))
        hi = step.astype(BF16)
        rest = step - hi.astype(F32)
        mid = rest.astype(BF16)
        low = (rest - mid.astype(F32)).astype(BF16)
        cum = dot1(hi, upto) + (dot1(mid, upto) + dot1(low, upto))
        count = cum.shape[0]
        total = jnp.broadcast_to(cum[:, CH - 1 : CH], (count, CH))
        columns = jnp.transpose(
            jnp.concatenate(
                [cum + jnp.log(beta), jnp.exp(total - cum), jnp.zeros((CH - 2 * count, CH), F32)], axis=0
            )
        )
        return beta, cum, jnp.exp(total), jnp.exp(cum), columns

    def weighted(t, kp, rows):
        kp = silu(kp)
        for h in range(2):
            lanes = slice(h * CH, (h + 1) * CH)
            kbuf[rows, lanes] = unit_rows(kp[:, lanes]).astype(BF16)

    def matrices(t, cum, columns):
        ms = []
        for n in range(per_seq):
            for h in range(2):
                k = part(kbuf, t, n, h)
                gram = lax.dot_general(k, k, ABT, preferred_element_type=F32)
                r = 2 * n + h
                ms.append(jnp.where(row > col, gram * jnp.exp(columns[:, r : r + 1] - cum[r : r + 1, :]), 0.0))
        return ms

    def part(buf, s, n, h):
        start = (s * per_seq + n) * CH
        return buf[start : start + CH, h * CH : (h + 1) * CH]

    rows_of = []
    ms = []
    for t in range(tiles):
        x_copy(t).wait()
        gt = jnp.concatenate([jnp.transpose(g) for g in halves(t, gatew, ABT, 2)], axis=1)
        count = 2
        size = tile // count
        kps = halves(t, wkbuf, AB, count)
        if t == 0:
            others[3].wait()
        vps = halves(t, wvbuf, AB, count)
        rows_of.append(scalars(t, gt))
        for i in range(count):
            weighted(t, kps[i], slice(t * tile + i * size, t * tile + (i + 1) * size))
        ms += matrices(t, rows_of[t][1], rows_of[t][4])
        for i in range(count):
            vbuf[t * tile + i * size : t * tile + (i + 1) * size, :] = silu(vps[i]).astype(BF16)

    items = [(s, n, h) for s in range(2) for n in range(per_seq) for h in range(2)]
    invs = inverses_of(ms)
    us = []
    for (s, n, h), inv in zip(items, invs):
        beta, _, _, _, columns = rows_of[s]
        r = 2 * n + h
        us.append(columns[:, 8 + r : 9 + r] * inv * beta[r : r + 1, :])
    pulls = [
        dot1(u * rows_of[s][3][2 * n + h : 2 * n + h + 1, :], part(kbuf, s, n, h)).astype(BF16)
        for (s, n, h), u in zip(items, us)
    ]
    freshs = [dot1(u, part(vbuf, s, n, h)).astype(BF16) for (s, n, h), u in zip(items, us)]
    boths = {
        (s, n, h): dot1(part(kbuf, s, n, h), jnp.concatenate([pull, fresh], axis=1), ATB)
        for (s, n, h), pull, fresh in zip(items, pulls, freshs)
    }
    maps = []
    for p in range(4):
        s, h = divmod(p, 2)
        parts = []
        for n in range(per_seq):
            c_row = rows_of[s][2][2 * n + h : 2 * n + h + 1, :]
            parts.append((c_row, boths[s, n, h][:, :CH], boths[s, n, h][:, CH:]))
        maps.append(parts)
    while len(maps[0]) > 1:
        maps = [[joined(m[i], m[i + 1], eye) for i in range(0, len(m), 2)] for m in maps]
    for p in range(4):
        c_row, drop, gain = maps[p][0]
        state[p, :CH, :] = c_row * eye - drop
        state[p, CH:, :] = gain

    for k, o in zip(SHIFTS, (o0, o1, o2, o3)):
        o[...] = state[lax.rem(here + k, 4)]


def segments_kernel(r0, r1, r2, r3, out, scr):
    here = lax.axis_index("sp_1")
    for k, ref in zip(SHIFTS, (r0, r1, r2, r3)):
        scr[lax.rem(here + 4 - k, 4)] = ref[...]
    state = jnp.concatenate([scr[0, :CH, :], scr[0, CH:, :]], axis=1)
    for t in range(1, 4):
        state = dot3(scr[t, :CH, :], state)
        state = state + jnp.concatenate([jnp.zeros((CH, CH), F32), scr[t, CH:, :]], axis=1)
    out[:CH, :] = state[:, :CH]
    out[CH:, :] = state[:, CH:]


def row_of(ref, s, h):
    two = ref[s].astype(F32)
    return jnp.sum(jnp.where(iota(two.shape, 0) == h, two, 0.0), axis=0, keepdims=True)


def new_token(query_ref, key_ref):
    pair = lax.axis_index("sp_1")
    s, h = lax.div(pair, 2), lax.rem(pair, 2)
    return s, h, unit_rows(row_of(query_ref, s, h)), unit_rows(row_of(key_ref, s, h))


def halves_kernel(own, other, query_ref, key_ref, mine, theirs, scr, amap, gain):
    part = lax.axis_index("sp_0")
    odd = lax.rem(part, 2)
    scr[odd] = own[...]
    scr[1 - odd] = other[...]
    _, _, qn, kn = new_token(query_ref, key_ref)
    both = dot3(scr[1, :CH, :], jnp.concatenate([scr[0, :CH, :], scr[0, CH:, :]], axis=1))
    amap[...] = both[:, :CH]
    gain[...] = both[:, CH:] + scr[1, CH:, :]

    @pl.when(part < 2)
    def _():
        mine[...] = gain[...]
        theirs[...] = gain[...]

    @pl.when(part >= 2)
    def _():
        reads = jnp.concatenate([kn, qn, jnp.zeros((6, CH), F32)], axis=0)
        through = dot3(reads, jnp.concatenate([amap[...], gain[...]], axis=1))
        for ref, owner in ((mine, part), (theirs, part - 2)):
            rows = pl.ds(pl.multiple_of(owner * ROWS, ROWS), ROWS)
            ref[:ROWS, :] = amap[rows, :]
            ref[ROWS : ROWS + 8, :] = through[:, :CH]
            ref[ROWS + 8 : 2 * ROWS + 8, :] = gain[rows, :]
            ref[2 * ROWS + 8 : 2 * ROWS + 16, :] = through[:, CH:]
            ref[2 * ROWS + 16 :, :] = jnp.zeros((CH - 2 * ROWS - 16, CH), F32)


def rows_kernel(mine, theirs, query_ref, key_ref, value_ref, gate_ref, gain_ref, out, scr):
    part = lax.axis_index("sp_0")
    right = jnp.where(part < 2, 0, 1)
    scr[right] = mine[...]
    scr[1 - right] = theirs[...]
    s, h, qn, kn = new_token(query_ref, key_ref)
    vn = row_of(value_ref, s, h)
    bn = 1.0 / (1.0 + jnp.exp(-jnp.full((1, CH), gate_ref[s, h], F32)))
    meet = jnp.sum(kn * qn, axis=1, keepdims=True)
    diagonal = iota((ROWS, CH), 1) == iota((ROWS, CH), 0) + part * ROWS
    k_col = jnp.sum(jnp.where(diagonal, jnp.broadcast_to(kn, (ROWS, CH)), 0.0), axis=1, keepdims=True)
    final = dot3(scr[1, : ROWS + 8, :], scr[0]) + scr[1, ROWS + 8 : 2 * ROWS + 16, :]
    missing = vn - final[ROWS : ROWS + 1, :]
    state = final[:ROWS, :] + k_col * (bn * missing)
    read = (final[ROWS + 1 : ROWS + 2, :] + bn * meet * missing) / math.sqrt(CH)
    scale = lax.rsqrt(jnp.mean(read * read, axis=-1, keepdims=True) + 1e-06)
    read_rows = jnp.broadcast_to(read * scale * gain_ref[...], (8, CH))
    for y in range(4):
        out[y, :8, :] = state[8 * y : 8 * y + 8, :]
        out[y, 8:, :] = read_rows


def finish_kernel(got, cache_ref, read_ref):
    for s in range(2):
        for h in range(2):
            cache_ref[s, h] = got[2 * s + h, :8, :].astype(BF16)
        read_ref[s] = jnp.concatenate([got[2 * s + h, 8:9, :] for h in range(2)], axis=0).astype(BF16)


def vmem(count):
    return [pl.BlockSpec(memory_space=pltpu.VMEM) for _ in range(count)]


def spread(arrays, axis):
    return [
        lax.ppermute(a, axis, [(i, (i + k) % 4) for i in range(4)]) if k else a
        for k, a in zip(SHIFTS, arrays)
    ]


def swap(array, axis, bit):
    return lax.ppermute(array, axis, [(i, i ^ bit) for i in range(4)])


def shards(
    tokens,
    key_matrix,
    value_matrix,
    gate_matrix,
    decay_matrix,
    gate_bias_offset,
    head_log_decay_rate,
    extra_log_decay,
    next_token_query,
    next_token_key,
    next_token_value,
    next_token_gate,
    readout_norm_gain,
):
    seqs, seg, width = tokens.shape
    cols = key_matrix.shape[1]
    tile = seg
    tiles = seqs * seg // tile
    chunks = seqs * seg // CH
    extra = jnp.transpose(extra_log_decay.reshape(chunks, CH, 2), (0, 2, 1))
    hbm = pl.BlockSpec(memory_space=pltpu.HBM)
    smem = pl.BlockSpec(memory_space=pltpu.SMEM)
    maps = pl.pallas_call(
        maps_kernel,
        out_shape=[jax.ShapeDtypeStruct((2 * CH, CH), F32)] * 4,
        in_specs=[hbm] * 8,
        out_specs=vmem(4),
        scratch_shapes=[
            pltpu.VMEM((tiles, tile, width), BF16),
            pltpu.VMEM((width, cols), BF16),
            pltpu.VMEM((width, cols), BF16),
            pltpu.VMEM((2 * gate_matrix.shape[1], width), BF16),
            pltpu.VMEM((chunks, 2, CH), F32),
            pltpu.SMEM(gate_bias_offset.shape, F32),
            pltpu.SMEM(head_log_decay_rate.shape, F32),
            pltpu.VMEM((seqs * seg, cols), BF16),
            pltpu.VMEM((seqs * seg, cols), BF16),
            pltpu.VMEM((4, 2 * CH, CH), F32),
            pltpu.SemaphoreType.DMA((tiles + 7,)),
        ],
        compiler_params=pltpu.CompilerParams(vmem_limit_bytes=24 * 2**20),
        name="maps",
    )(
        *(
            pltpu.with_memory_space_constraint(a, pltpu.HBM)
            for a in (
                tokens,
                key_matrix,
                value_matrix,
                gate_matrix.T,
                decay_matrix.T,
                gate_bias_offset,
                head_log_decay_rate,
                extra,
            )
        )
    )
    small = pltpu.CompilerParams(vmem_limit_bytes=8 * 2**20)
    segment = pl.pallas_call(
        segments_kernel,
        out_shape=jax.ShapeDtypeStruct((2 * CH, CH), F32),
        in_specs=vmem(4),
        out_specs=vmem(1)[0],
        scratch_shapes=[pltpu.VMEM((4, 2 * CH, CH), F32)],
        compiler_params=small,
        name="segments",
    )(*spread(maps, "sp_1"))
    mine, theirs = pl.pallas_call(
        halves_kernel,
        out_shape=[jax.ShapeDtypeStruct((CH, CH), F32)] * 2,
        in_specs=vmem(4),
        out_specs=vmem(2),
        scratch_shapes=[
            pltpu.VMEM((2, 2 * CH, CH), F32),
            pltpu.VMEM((CH, CH), F32),
            pltpu.VMEM((CH, CH), F32),
        ],
        compiler_params=small,
        name="halves",
    )(segment, swap(segment, "sp_0", 1), next_token_query, next_token_key)
    rows = pl.pallas_call(
        rows_kernel,
        out_shape=jax.ShapeDtypeStruct((4, 16, CH), F32),
        in_specs=[*vmem(5), smem, *vmem(1)],
        out_specs=vmem(1)[0],
        scratch_shapes=[pltpu.VMEM((2, CH, CH), F32)],
        compiler_params=small,
        name="rows",
    )(
        mine,
        swap(theirs, "sp_0", 2),
        next_token_query,
        next_token_key,
        next_token_value,
        next_token_gate,
        readout_norm_gain.reshape(1, CH),
    )
    got = lax.all_to_all(rows, "sp_1", 0, 0, tiled=True)
    return pl.pallas_call(
        finish_kernel,
        out_shape=[
            jax.ShapeDtypeStruct((2, 2, 8, CH), BF16),
            jax.ShapeDtypeStruct((2, 2, CH), BF16),
        ],
        in_specs=vmem(1),
        out_specs=vmem(2),
        compiler_params=small,
        name="finish",
    )(got)


def solution(mesh):
    finer = Mesh(
        mesh.devices.reshape(mesh.shape["gr"], 4, 4, mesh.shape["tp"]), ("gr", "sp_0", "sp_1", "tp")
    )
    in_specs = (
        P("gr", SP, None),
        P(None, "tp"),
        P(None, "tp"),
        P(),
        P(),
        P(),
        P(),
        P("gr", SP, "tp"),
        P("gr", "tp", None),
        P("gr", "tp", None),
        P("gr", "tp", None),
        P("gr", "tp"),
        P(),
    )
    out_specs = (P("gr", "tp", SP, None), P("gr", "tp", None))
    return jax.shard_map(
        shards, mesh=finer, in_specs=in_specs, out_specs=out_specs, check_vma=False
    )
```

```python
import math

import jax
import jax.numpy as jnp
from jax import lax
from jax.experimental import pallas as pl
from jax.experimental.pallas import tpu as pltpu
from jax.sharding import Mesh
from jax.sharding import PartitionSpec as P

SP = ("sp_0", "sp_1")
CH = 128
ROWS = 32
SHIFTS = (0, 2, 3, 1)
F32 = jnp.float32
BF16 = jnp.bfloat16
AB = (((1,), (0,)), ((), ()))
ABT = (((1,), (1,)), ((), ()))
ATB = (((0,), (0,)), ((), ()))


def dot1(a, b, dims=AB):
    return lax.dot_general(a.astype(BF16), b.astype(BF16), dims, preferred_element_type=F32)


def split(a):
    hi = a.astype(BF16)
    return hi, (a - hi.astype(F32)).astype(BF16)


def dot3(a, b, dims=AB):
    ah, al = split(a)
    bh, bl = split(b)
    return dot1(ah, bh, dims) + (dot1(ah, bl, dims) + dot1(al, bh, dims))


def iota(shape, dim):
    return lax.broadcasted_iota(jnp.int32, shape, dim)


def unit_rows(a):
    return a * lax.rsqrt(jnp.sum(a * a, axis=-1, keepdims=True) + 1e-06)


def silu(a):
    return a * (1.0 / (1.0 + jnp.exp(-a)))


def inverses_of(m_mats):
    row = iota((CH, CH), 0)
    col = iota((CH, CH), 1)
    eye = jnp.where(row == col, 1.0, 0.0)
    near = row // 16 == col // 16
    p1s = [jnp.where(near, -m, 0.0) for m in m_mats]
    invs = [eye + p for p in p1s]
    pows = [p.astype(BF16) for p in p1s]
    pows = [dot1(p, p).astype(BF16) for p in pows]
    for last in (False, False, True):
        if last:
            adds = [dot1(p, i) for p, i in zip(pows, invs)]
        else:
            both = [dot1(p, jnp.concatenate([p, i.astype(BF16)], axis=1)) for p, i in zip(pows, invs)]
            adds = [x[:, CH:] for x in both]
            pows = [x[:, :CH].astype(BF16) for x in both]
        invs = [i + x for i, x in zip(invs, adds)]
    for b in (16, 32, 64):
        lower = [slice(s + b, s + 2 * b) for s in range(0, CH, 2 * b)]

        def gather(rows_of):
            return jnp.concatenate([rows_of(r) for r in lower], axis=0)

        m_rows = [
            gather(lambda r: jnp.where(col[r, :] // b == (r.start // b - 1), m[r, :], 0.0))
            for m in m_mats
        ]
        t_rows = [gather(lambda r: i[r, :]) for i in invs]
        uppers = []
        for i in invs:
            pieces = []
            for r in lower:
                pieces += [i[r.start - b : r.start, :].astype(BF16), jnp.zeros((b, CH), BF16)]
            uppers.append(jnp.concatenate(pieces, axis=0))
        ys = [dot1(m, i).astype(BF16) for m, i in zip(m_rows, uppers)]
        spread_out = []
        for y in ys:
            pieces = []
            for g in range(len(lower)):
                pieces += [jnp.zeros((b, CH), BF16), y[g * b : (g + 1) * b, :]]
            spread_out.append(jnp.concatenate(pieces, axis=0))
        news = [t - dot1(t, y) for t, y in zip(t_rows, spread_out)]
        joined = []
        for i, new in zip(invs, news):
            pieces = []
            for g, r in enumerate(lower):
                pieces += [i[r.start - b : r.start, :], new[g * b : (g + 1) * b, :]]
            joined.append(jnp.concatenate(pieces, axis=0))
        invs = joined
    return invs


def joined(first, second, eye):
    c1, d1, b1 = first
    c2, d2, b2 = second
    moved = dot1(d2, jnp.concatenate([c1 * eye - d1, b1], axis=1))
    return c1 * c2, c2 * d1 + moved[:, :CH], c2 * b1 - moved[:, CH:] + b2


def maps_kernel(
    x_hbm, wk_hbm, wv_hbm, gate_hbm, decay_hbm, bias_hbm, rate_hbm, extra_hbm,
    o0, o1, o2, o3,
    xbuf, wkbuf, wvbuf, gatew, extra, bias_ref, rate_ref, kbuf, vbuf, state, sems,
):
    tiles, tile, width = xbuf.shape
    half = tile // 2
    first_head = lax.axis_index("tp") * 2
    here = lax.axis_index("sp_1")
    per_seq = kbuf.shape[0] // (2 * CH)
    heads = gate_hbm.shape[0]
    moves = [
        (gate_hbm, gatew.at[pl.ds(0, heads)]),
        (decay_hbm, gatew.at[pl.ds(heads, heads)]),
        (bias_hbm, bias_ref),
        (rate_hbm, rate_ref),
        (extra_hbm, extra),
    ]
    small = len(moves)
    for t in range(tiles):
        for i in range(2):
            rows = pl.ds(i * half, half)
            moves.append((x_hbm.at[t, rows], xbuf.at[t, rows]))
            if t == 0:
                moves.append(((wk_hbm, wkbuf), (wv_hbm, wvbuf))[i])
    copies = [pltpu.make_async_copy(src, dst, sems.at[i]) for i, (src, dst) in enumerate(moves)]
    for c in copies:
        c.start()
    for c in copies[:small]:
        c.wait()
    arrivals = copies[small:]
    pick = iota((heads, tile), 0)
    odd = iota((2, tile), 0) == 1
    bias = jnp.where(odd, bias_ref[first_head + 1], bias_ref[first_head])
    rate = jnp.exp(jnp.where(odd, rate_ref[first_head + 1], rate_ref[first_head]))
    row = iota((CH, CH), 0)
    col = iota((CH, CH), 1)
    eye = jnp.where(row == col, 1.0, 0.0)
    upto = jnp.where(row <= col, 1.0, 0.0).astype(BF16)

    def times(t, i, weights, dims=AB):
        x = xbuf[t, i * half : (i + 1) * half]
        return lax.dot_general(x, weights[...], dims, preferred_element_type=F32)

    def scalars(t, gt):
        picked = [
            jnp.sum(jnp.where(pick == first_head + h, part, 0.0), axis=0, keepdims=True)
            for part in (gt[:heads], gt[heads:])
            for h in range(2)
        ]
        z = jnp.concatenate(picked[2:], axis=0)
        soft = jnp.maximum(z, 0.0) + jnp.log1p(jnp.exp(-jnp.abs(z)))
        gate = jnp.concatenate(picked[:2], axis=0) + bias
        steps, gates = [], []
        for n in range(per_seq):
            lanes = slice(n * CH, (n + 1) * CH)
            steps.append(extra[t * per_seq + n] - rate[:, lanes] * soft[:, lanes])
            gates.append(gate[:, lanes])
        step = jnp.concatenate(steps, axis=0)
        beta = 1.0 / (1.0 + jnp.exp(-jnp.concatenate(gates, axis=0)))
        hi = step.astype(BF16)
        rest = step - hi.astype(F32)
        mid = rest.astype(BF16)
        low = (rest - mid.astype(F32)).astype(BF16)
        cum = dot1(hi, upto) + (dot1(mid, upto) + dot1(low, upto))
        count = cum.shape[0]
        total = jnp.broadcast_to(cum[:, CH - 1 : CH], (count, CH))
        columns = jnp.transpose(
            jnp.concatenate(
                [cum + jnp.log(beta), jnp.exp(total - cum), jnp.zeros((CH - 2 * count, CH), F32)], axis=0
            )
        )
        return beta, cum, jnp.exp(total), jnp.exp(cum), columns

    def weighted(t, kp, rows):
        kp = silu(kp)
        for h in range(2):
            lanes = slice(h * CH, (h + 1) * CH)
            kbuf[rows, lanes] = unit_rows(kp[:, lanes]).astype(BF16)

    def matrices(t, cum, columns):
        ms = []
        for n in range(per_seq):
            for h in range(2):
                k = part(kbuf, t, n, h)
                gram = lax.dot_general(k, k, ABT, preferred_element_type=F32)
                r = 2 * n + h
                ms.append(jnp.where(row > col, gram * jnp.exp(columns[:, r : r + 1] - cum[r : r + 1, :]), 0.0))
        return ms

    def part(buf, s, n, h):
        start = (s * per_seq + n) * CH
        return buf[start : start + CH, h * CH : (h + 1) * CH]

    def keys(t, i, kp):
        weighted(t, kp, slice(t * tile + i * half, t * tile + (i + 1) * half))

    def values(t, i, vp):
        vbuf[t * tile + i * half : t * tile + (i + 1) * half, :] = silu(vp).astype(BF16)

    def rows_from(t, gts):
        return scalars(t, jnp.concatenate([jnp.transpose(g) for g in gts], axis=1))

    x00, wk, x01, wv, x10, x11 = arrivals
    x00.wait()
    wk.wait()
    g00 = times(0, 0, gatew, ABT)
    k00 = times(0, 0, wkbuf)
    x01.wait()
    g01 = times(0, 1, gatew, ABT)
    k01 = times(0, 1, wkbuf)
    keys(0, 0, k00)
    wv.wait()
    v00 = times(0, 0, wvbuf)
    v01 = times(0, 1, wvbuf)
    keys(0, 1, k01)
    x10.wait()
    x11.wait()
    g10 = times(1, 0, gatew, ABT)
    k10 = times(1, 0, wkbuf)
    rows_of = [rows_from(0, (g00, g01))]
    g11 = times(1, 1, gatew, ABT)
    k11 = times(1, 1, wkbuf)
    values(0, 0, v00)
    values(0, 1, v01)
    rows_of.append(rows_from(1, (g10, g11)))
    keys(1, 0, k10)
    v10 = times(1, 0, wvbuf)
    v11 = times(1, 1, wvbuf)
    ms = matrices(0, rows_of[0][1], rows_of[0][4])
    keys(1, 1, k11)
    ms += matrices(1, rows_of[1][1], rows_of[1][4])
    values(1, 0, v10)
    values(1, 1, v11)

    items = [(s, n, h) for s in range(2) for n in range(per_seq) for h in range(2)]
    invs = inverses_of(ms)
    us = []
    for (s, n, h), inv in zip(items, invs):
        beta, _, _, _, columns = rows_of[s]
        r = 2 * n + h
        us.append(columns[:, 8 + r : 9 + r] * inv * beta[r : r + 1, :])
    pulls = [
        dot1(u * rows_of[s][3][2 * n + h : 2 * n + h + 1, :], part(kbuf, s, n, h)).astype(BF16)
        for (s, n, h), u in zip(items, us)
    ]
    freshs = [dot1(u, part(vbuf, s, n, h)).astype(BF16) for (s, n, h), u in zip(items, us)]
    boths = {
        (s, n, h): dot1(part(kbuf, s, n, h), jnp.concatenate([pull, fresh], axis=1), ATB)
        for (s, n, h), pull, fresh in zip(items, pulls, freshs)
    }
    maps = []
    for p in range(4):
        s, h = divmod(p, 2)
        parts = []
        for n in range(per_seq):
            c_row = rows_of[s][2][2 * n + h : 2 * n + h + 1, :]
            parts.append((c_row, boths[s, n, h][:, :CH], boths[s, n, h][:, CH:]))
        maps.append(parts)
    while len(maps[0]) > 1:
        maps = [[joined(m[i], m[i + 1], eye) for i in range(0, len(m), 2)] for m in maps]
    for p in range(4):
        c_row, drop, gain = maps[p][0]
        state[p, :CH, :] = c_row * eye - drop
        state[p, CH:, :] = gain

    for k, o in zip(SHIFTS, (o0, o1, o2, o3)):
        o[...] = state[lax.rem(here + k, 4)]


def segments_kernel(r0, r1, r2, r3, out, scr):
    here = lax.axis_index("sp_1")
    for k, ref in zip(SHIFTS, (r0, r1, r2, r3)):
        scr[lax.rem(here + 4 - k, 4)] = ref[...]
    state = jnp.concatenate([scr[0, :CH, :], scr[0, CH:, :]], axis=1)
    for t in range(1, 4):
        state = dot3(scr[t, :CH, :], state)
        state = state + jnp.concatenate([jnp.zeros((CH, CH), F32), scr[t, CH:, :]], axis=1)
    out[:CH, :] = state[:, :CH]
    out[CH:, :] = state[:, CH:]


def row_of(ref, s, h):
    two = ref[s].astype(F32)
    return jnp.sum(jnp.where(iota(two.shape, 0) == h, two, 0.0), axis=0, keepdims=True)


def new_token(query_ref, key_ref):
    pair = lax.axis_index("sp_1")
    s, h = lax.div(pair, 2), lax.rem(pair, 2)
    return s, h, unit_rows(row_of(query_ref, s, h)), unit_rows(row_of(key_ref, s, h))


def halves_kernel(own, other, query_ref, key_ref, mine, theirs, scr, amap, gain):
    part = lax.axis_index("sp_0")
    odd = lax.rem(part, 2)
    scr[odd] = own[...]
    scr[1 - odd] = other[...]
    _, _, qn, kn = new_token(query_ref, key_ref)
    both = dot3(scr[1, :CH, :], jnp.concatenate([scr[0, :CH, :], scr[0, CH:, :]], axis=1))
    amap[...] = both[:, :CH]
    gain[...] = both[:, CH:] + scr[1, CH:, :]

    @pl.when(part < 2)
    def _():
        mine[...] = gain[...]
        theirs[...] = gain[...]

    @pl.when(part >= 2)
    def _():
        reads = jnp.concatenate([kn, qn, jnp.zeros((6, CH), F32)], axis=0)
        through = dot3(reads, jnp.concatenate([amap[...], gain[...]], axis=1))
        for ref, owner in ((mine, part), (theirs, part - 2)):
            rows = pl.ds(pl.multiple_of(owner * ROWS, ROWS), ROWS)
            ref[:ROWS, :] = amap[rows, :]
            ref[ROWS : ROWS + 8, :] = through[:, :CH]
            ref[ROWS + 8 : 2 * ROWS + 8, :] = gain[rows, :]
            ref[2 * ROWS + 8 : 2 * ROWS + 16, :] = through[:, CH:]
            ref[2 * ROWS + 16 :, :] = jnp.zeros((CH - 2 * ROWS - 16, CH), F32)


def rows_kernel(mine, theirs, query_ref, key_ref, value_ref, gate_ref, gain_ref, out, scr):
    part = lax.axis_index("sp_0")
    right = jnp.where(part < 2, 0, 1)
    scr[right] = mine[...]
    scr[1 - right] = theirs[...]
    s, h, qn, kn = new_token(query_ref, key_ref)
    vn = row_of(value_ref, s, h)
    bn = 1.0 / (1.0 + jnp.exp(-jnp.full((1, CH), gate_ref[s, h], F32)))
    meet = jnp.sum(kn * qn, axis=1, keepdims=True)
    diagonal = iota((ROWS, CH), 1) == iota((ROWS, CH), 0) + part * ROWS
    k_col = jnp.sum(jnp.where(diagonal, jnp.broadcast_to(kn, (ROWS, CH)), 0.0), axis=1, keepdims=True)
    final = dot3(scr[1, : ROWS + 8, :], scr[0]) + scr[1, ROWS + 8 : 2 * ROWS + 16, :]
    missing = vn - final[ROWS : ROWS + 1, :]
    state = final[:ROWS, :] + k_col * (bn * missing)
    read = (final[ROWS + 1 : ROWS + 2, :] + bn * meet * missing) / math.sqrt(CH)
    scale = lax.rsqrt(jnp.mean(read * read, axis=-1, keepdims=True) + 1e-06)
    read_rows = jnp.broadcast_to(read * scale * gain_ref[...], (8, CH))
    for y in range(4):
        out[y, :8, :] = state[8 * y : 8 * y + 8, :]
        out[y, 8:, :] = read_rows


def finish_kernel(got, cache_ref, read_ref):
    for s in range(2):
        for h in range(2):
            cache_ref[s, h] = got[2 * s + h, :8, :].astype(BF16)
        read_ref[s] = jnp.concatenate([got[2 * s + h, 8:9, :] for h in range(2)], axis=0).astype(BF16)


def vmem(count):
    return [pl.BlockSpec(memory_space=pltpu.VMEM) for _ in range(count)]


def spread(arrays, axis):
    return [
        lax.ppermute(a, axis, [(i, (i + k) % 4) for i in range(4)]) if k else a
        for k, a in zip(SHIFTS, arrays)
    ]


def swap(array, axis, bit):
    return lax.ppermute(array, axis, [(i, i ^ bit) for i in range(4)])


def shards(
    tokens,
    key_matrix,
    value_matrix,
    gate_matrix,
    decay_matrix,
    gate_bias_offset,
    head_log_decay_rate,
    extra_log_decay,
    next_token_query,
    next_token_key,
    next_token_value,
    next_token_gate,
    readout_norm_gain,
):
    seqs, seg, width = tokens.shape
    cols = key_matrix.shape[1]
    tile = seg
    tiles = seqs * seg // tile
    chunks = seqs * seg // CH
    extra = jnp.transpose(extra_log_decay.reshape(chunks, CH, 2), (0, 2, 1))
    hbm = pl.BlockSpec(memory_space=pltpu.HBM)
    smem = pl.BlockSpec(memory_space=pltpu.SMEM)
    maps = pl.pallas_call(
        maps_kernel,
        out_shape=[jax.ShapeDtypeStruct((2 * CH, CH), F32)] * 4,
        in_specs=[hbm] * 8,
        out_specs=vmem(4),
        scratch_shapes=[
            pltpu.VMEM((tiles, tile, width), BF16),
            pltpu.VMEM((width, cols), BF16),
            pltpu.VMEM((width, cols), BF16),
            pltpu.VMEM((2 * gate_matrix.shape[1], width), BF16),
            pltpu.VMEM((chunks, 2, CH), F32),
            pltpu.SMEM(gate_bias_offset.shape, F32),
            pltpu.SMEM(head_log_decay_rate.shape, F32),
            pltpu.VMEM((seqs * seg, cols), BF16),
            pltpu.VMEM((seqs * seg, cols), BF16),
            pltpu.VMEM((4, 2 * CH, CH), F32),
            pltpu.SemaphoreType.DMA((11,)),
        ],
        compiler_params=pltpu.CompilerParams(vmem_limit_bytes=24 * 2**20),
        name="maps",
    )(
        *(
            pltpu.with_memory_space_constraint(a, pltpu.HBM)
            for a in (
                tokens,
                key_matrix,
                value_matrix,
                gate_matrix.T,
                decay_matrix.T,
                gate_bias_offset,
                head_log_decay_rate,
                extra,
            )
        )
    )
    small = pltpu.CompilerParams(vmem_limit_bytes=8 * 2**20)
    segment = pl.pallas_call(
        segments_kernel,
        out_shape=jax.ShapeDtypeStruct((2 * CH, CH), F32),
        in_specs=vmem(4),
        out_specs=vmem(1)[0],
        scratch_shapes=[pltpu.VMEM((4, 2 * CH, CH), F32)],
        compiler_params=small,
        name="segments",
    )(*spread(maps, "sp_1"))
    mine, theirs = pl.pallas_call(
        halves_kernel,
        out_shape=[jax.ShapeDtypeStruct((CH, CH), F32)] * 2,
        in_specs=vmem(4),
        out_specs=vmem(2),
        scratch_shapes=[
            pltpu.VMEM((2, 2 * CH, CH), F32),
            pltpu.VMEM((CH, CH), F32),
            pltpu.VMEM((CH, CH), F32),
        ],
        compiler_params=small,
        name="halves",
    )(segment, swap(segment, "sp_0", 1), next_token_query, next_token_key)
    rows = pl.pallas_call(
        rows_kernel,
        out_shape=jax.ShapeDtypeStruct((4, 16, CH), F32),
        in_specs=[*vmem(5), smem, *vmem(1)],
        out_specs=vmem(1)[0],
        scratch_shapes=[pltpu.VMEM((2, CH, CH), F32)],
        compiler_params=small,
        name="rows",
    )(
        mine,
        swap(theirs, "sp_0", 2),
        next_token_query,
        next_token_key,
        next_token_value,
        next_token_gate,
        readout_norm_gain.reshape(1, CH),
    )
    got = lax.all_to_all(rows, "sp_1", 0, 0, tiled=True)
    return pl.pallas_call(
        finish_kernel,
        out_shape=[
            jax.ShapeDtypeStruct((2, 2, 8, CH), BF16),
            jax.ShapeDtypeStruct((2, 2, CH), BF16),
        ],
        in_specs=vmem(1),
        out_specs=vmem(2),
        compiler_params=small,
        name="finish",
    )(got)


def solution(mesh):
    finer = Mesh(
        mesh.devices.reshape(mesh.shape["gr"], 4, 4, mesh.shape["tp"]), ("gr", "sp_0", "sp_1", "tp")
    )
    in_specs = (
        P("gr", SP, None),
        P(None, "tp"),
        P(None, "tp"),
        P(),
        P(),
        P(),
        P(),
        P("gr", SP, "tp"),
        P("gr", "tp", None),
        P("gr", "tp", None),
        P("gr", "tp", None),
        P("gr", "tp"),
        P(),
    )
    out_specs = (P("gr", "tp", SP, None), P("gr", "tp", None))
    return jax.shard_map(
        shards, mesh=finer, in_specs=in_specs, out_specs=out_specs, check_vma=False
    )
```

```python
import math

import jax
import jax.numpy as jnp
from jax import lax
from jax.experimental import pallas as pl
from jax.experimental.pallas import tpu as pltpu
from jax.sharding import Mesh
from jax.sharding import PartitionSpec as P

SP = ("sp_0", "sp_1")
CH = 128
ROWS = 32
SHIFTS = (0, 2, 3, 1)
F32 = jnp.float32
BF16 = jnp.bfloat16
AB = (((1,), (0,)), ((), ()))
ABT = (((1,), (1,)), ((), ()))
ATB = (((0,), (0,)), ((), ()))


def dot1(a, b, dims=AB):
    return lax.dot_general(a.astype(BF16), b.astype(BF16), dims, preferred_element_type=F32)


def split(a):
    hi = a.astype(BF16)
    return hi, (a - hi.astype(F32)).astype(BF16)


def dot3(a, b, dims=AB):
    ah, al = split(a)
    bh, bl = split(b)
    return dot1(ah, bh, dims) + (dot1(ah, bl, dims) + dot1(al, bh, dims))


def iota(shape, dim):
    return lax.broadcasted_iota(jnp.int32, shape, dim)


def unit_rows(a):
    return a * lax.rsqrt(jnp.sum(a * a, axis=-1, keepdims=True) + 1e-06)


def silu(a):
    return a * (1.0 / (1.0 + jnp.exp(-a)))


def inverses_of(m_mats):
    row = iota((CH, CH), 0)
    col = iota((CH, CH), 1)
    eye = jnp.where(row == col, 1.0, 0.0)
    near = row // 16 == col // 16
    p1s = [jnp.where(near, -m, 0.0) for m in m_mats]
    invs = [eye + p for p in p1s]
    pows = [p.astype(BF16) for p in p1s]
    pows = [dot1(p, p).astype(BF16) for p in pows]
    for last in (False, False, True):
        if last:
            adds = [dot1(p, i) for p, i in zip(pows, invs)]
        else:
            both = [dot1(p, jnp.concatenate([p, i.astype(BF16)], axis=1)) for p, i in zip(pows, invs)]
            adds = [x[:, CH:] for x in both]
            pows = [x[:, :CH].astype(BF16) for x in both]
        invs = [i + x for i, x in zip(invs, adds)]
    for b in (16, 32, 64):
        lower = [slice(s + b, s + 2 * b) for s in range(0, CH, 2 * b)]

        def gather(rows_of):
            return jnp.concatenate([rows_of(r) for r in lower], axis=0)

        m_rows = [
            gather(lambda r: jnp.where(col[r, :] // b == (r.start // b - 1), m[r, :], 0.0))
            for m in m_mats
        ]
        t_rows = [gather(lambda r: i[r, :]) for i in invs]
        uppers = []
        for i in invs:
            pieces = []
            for r in lower:
                pieces += [i[r.start - b : r.start, :].astype(BF16), jnp.zeros((b, CH), BF16)]
            uppers.append(jnp.concatenate(pieces, axis=0))
        ys = [dot1(m, i).astype(BF16) for m, i in zip(m_rows, uppers)]
        spread_out = []
        for y in ys:
            pieces = []
            for g in range(len(lower)):
                pieces += [jnp.zeros((b, CH), BF16), y[g * b : (g + 1) * b, :]]
            spread_out.append(jnp.concatenate(pieces, axis=0))
        news = [t - dot1(t, y) for t, y in zip(t_rows, spread_out)]
        joined = []
        for i, new in zip(invs, news):
            pieces = []
            for g, r in enumerate(lower):
                pieces += [i[r.start - b : r.start, :], new[g * b : (g + 1) * b, :]]
            joined.append(jnp.concatenate(pieces, axis=0))
        invs = joined
    return invs


def joined(first, second, eye):
    c1, d1, b1 = first
    c2, d2, b2 = second
    moved = dot1(d2, jnp.concatenate([c1 * eye - d1, b1], axis=1))
    return c1 * c2, c2 * d1 + moved[:, :CH], c2 * b1 - moved[:, CH:] + b2


def maps_kernel(
    x_hbm, wk_hbm, wv_hbm, gate_hbm, decay_hbm, bias_hbm, rate_hbm, extra_hbm,
    o0, o1, o2, o3,
    xbuf, wkbuf, wvbuf, gatew, extra, bias_ref, rate_ref, kbuf, vbuf, state, sems,
):
    tiles, tile, width = xbuf.shape
    half = tile // 2
    first_head = lax.axis_index("tp") * 2
    here = lax.axis_index("sp_1")
    per_seq = kbuf.shape[0] // (2 * CH)
    heads = gate_hbm.shape[0]
    moves = [
        (gate_hbm, gatew.at[pl.ds(0, heads)]),
        (decay_hbm, gatew.at[pl.ds(heads, heads)]),
        (bias_hbm, bias_ref),
        (rate_hbm, rate_ref),
        (extra_hbm, extra),
    ]
    small = len(moves)
    for t in range(tiles):
        for i in range(2):
            rows = pl.ds(i * half, half)
            moves.append((x_hbm.at[t, rows], xbuf.at[t, rows]))
            if t == 0:
                moves.append(((wk_hbm, wkbuf), (wv_hbm, wvbuf))[i])
    copies = [pltpu.make_async_copy(src, dst, sems.at[i]) for i, (src, dst) in enumerate(moves)]
    for c in copies:
        c.start()
    for c in copies[:small]:
        c.wait()
    arrivals = copies[small:]
    pick = iota((heads, tile), 0)
    odd = iota((2, tile), 0) == 1
    bias = jnp.where(odd, bias_ref[first_head + 1], bias_ref[first_head])
    rate = jnp.exp(jnp.where(odd, rate_ref[first_head + 1], rate_ref[first_head]))
    row = iota((CH, CH), 0)
    col = iota((CH, CH), 1)
    eye = jnp.where(row == col, 1.0, 0.0)
    upto = jnp.where(row <= col, 1.0, 0.0).astype(BF16)

    def times(t, i, weights, dims=AB):
        x = xbuf[t, i * half : (i + 1) * half]
        return lax.dot_general(x, weights[...], dims, preferred_element_type=F32)

    def scalars(t, gt):
        picked = [
            jnp.sum(jnp.where(pick == first_head + h, part, 0.0), axis=0, keepdims=True)
            for part in (gt[:heads], gt[heads:])
            for h in range(2)
        ]
        z = jnp.concatenate(picked[2:], axis=0)
        soft = jnp.maximum(z, 0.0) + jnp.log1p(jnp.exp(-jnp.abs(z)))
        gate = jnp.concatenate(picked[:2], axis=0) + bias
        steps, gates = [], []
        for n in range(per_seq):
            lanes = slice(n * CH, (n + 1) * CH)
            steps.append(extra[t * per_seq + n] - rate[:, lanes] * soft[:, lanes])
            gates.append(gate[:, lanes])
        step = jnp.concatenate(steps, axis=0)
        beta = 1.0 / (1.0 + jnp.exp(-jnp.concatenate(gates, axis=0)))
        hi = step.astype(BF16)
        rest = step - hi.astype(F32)
        mid = rest.astype(BF16)
        low = (rest - mid.astype(F32)).astype(BF16)
        cum = dot1(hi, upto) + (dot1(mid, upto) + dot1(low, upto))
        count = cum.shape[0]
        total = jnp.broadcast_to(cum[:, CH - 1 : CH], (count, CH))
        columns = jnp.transpose(
            jnp.concatenate(
                [cum + jnp.log(beta), jnp.exp(total - cum), jnp.zeros((CH - 2 * count, CH), F32)], axis=0
            )
        )
        return beta, cum, jnp.exp(total), jnp.exp(cum), columns

    def weighted(t, kp, rows):
        kp = silu(kp)
        for h in range(2):
            lanes = slice(h * CH, (h + 1) * CH)
            kbuf[rows, lanes] = unit_rows(kp[:, lanes]).astype(BF16)

    def matrices(t, cum, columns):
        ms = []
        for n in range(per_seq):
            for h in range(2):
                k = part(kbuf, t, n, h)
                gram = lax.dot_general(k, k, ABT, preferred_element_type=F32)
                r = 2 * n + h
                ms.append(jnp.where(row > col, gram * jnp.exp(columns[:, r : r + 1] - cum[r : r + 1, :]), 0.0))
        return ms

    def part(buf, s, n, h):
        start = (s * per_seq + n) * CH
        return buf[start : start + CH, h * CH : (h + 1) * CH]

    def keys(t, i, kp):
        weighted(t, kp, slice(t * tile + i * half, t * tile + (i + 1) * half))

    def values(t, i, vp):
        vbuf[t * tile + i * half : t * tile + (i + 1) * half, :] = silu(vp).astype(BF16)

    def rows_from(t, gts):
        return scalars(t, jnp.concatenate([jnp.transpose(g) for g in gts], axis=1))

    x00, wk, x01, wv, x10, x11 = arrivals
    x00.wait()
    wk.wait()
    g00 = times(0, 0, gatew, ABT)
    k00 = times(0, 0, wkbuf)
    x01.wait()
    g01 = times(0, 1, gatew, ABT)
    k01 = times(0, 1, wkbuf)
    keys(0, 0, k00)
    wv.wait()
    v00 = times(0, 0, wvbuf)
    v01 = times(0, 1, wvbuf)
    keys(0, 1, k01)
    x10.wait()
    x11.wait()
    g10 = times(1, 0, gatew, ABT)
    k10 = times(1, 0, wkbuf)
    rows_of = [rows_from(0, (g00, g01))]
    g11 = times(1, 1, gatew, ABT)
    k11 = times(1, 1, wkbuf)
    values(0, 0, v00)
    values(0, 1, v01)
    rows_of.append(rows_from(1, (g10, g11)))
    keys(1, 0, k10)
    v10 = times(1, 0, wvbuf)
    v11 = times(1, 1, wvbuf)
    ms = matrices(0, rows_of[0][1], rows_of[0][4])
    keys(1, 1, k11)
    ms += matrices(1, rows_of[1][1], rows_of[1][4])
    values(1, 0, v10)
    values(1, 1, v11)

    items = [(s, n, h) for s in range(2) for n in range(per_seq) for h in range(2)]
    invs = inverses_of(ms)
    us = []
    for (s, n, h), inv in zip(items, invs):
        beta, _, _, _, columns = rows_of[s]
        r = 2 * n + h
        us.append(columns[:, 8 + r : 9 + r] * inv * beta[r : r + 1, :])
    pulls = [
        dot1(u * rows_of[s][3][2 * n + h : 2 * n + h + 1, :], part(kbuf, s, n, h)).astype(BF16)
        for (s, n, h), u in zip(items, us)
    ]
    freshs = [dot1(u, part(vbuf, s, n, h)).astype(BF16) for (s, n, h), u in zip(items, us)]
    boths = {
        (s, n, h): dot1(part(kbuf, s, n, h), jnp.concatenate([pull, fresh], axis=1), ATB)
        for (s, n, h), pull, fresh in zip(items, pulls, freshs)
    }
    maps = []
    for p in range(4):
        s, h = divmod(p, 2)
        parts = []
        for n in range(per_seq):
            c_row = rows_of[s][2][2 * n + h : 2 * n + h + 1, :]
            parts.append((c_row, boths[s, n, h][:, :CH], boths[s, n, h][:, CH:]))
        maps.append(parts)
    while len(maps[0]) > 1:
        maps = [[joined(m[i], m[i + 1], eye) for i in range(0, len(m), 2)] for m in maps]
    for p in range(4):
        c_row, drop, gain = maps[p][0]
        state[p, :CH, :] = c_row * eye - drop
        state[p, CH:, :] = gain

    for k, o in zip(SHIFTS, (o0, o1, o2, o3)):
        o[...] = state[lax.rem(here + k, 4)]


def after(first, second):
    both = dot3(second[0], jnp.concatenate(first, axis=1))
    return both[:, :CH], both[:, CH:] + second[1]


def segments_kernel(r0, r1, r2, r3, out, scr):
    here = lax.axis_index("sp_1")
    for k, ref in zip(SHIFTS, (r0, r1, r2, r3)):
        scr[lax.rem(here + 4 - k, 4)] = ref[...]
    maps = [(scr[t, :CH, :], scr[t, CH:, :]) for t in range(4)]
    while len(maps) > 1:
        maps = [after(maps[i], maps[i + 1]) for i in range(0, len(maps), 2)]
    out[:CH, :], out[CH:, :] = maps[0]


def row_of(ref, s, h):
    two = ref[s].astype(F32)
    return jnp.sum(jnp.where(iota(two.shape, 0) == h, two, 0.0), axis=0, keepdims=True)


def token_kernel(query_ref, key_ref, value_ref, gate_ref, out):
    part = lax.axis_index("sp_0")
    pair = lax.axis_index("sp_1")
    s, h = lax.div(pair, 2), lax.rem(pair, 2)
    kn = unit_rows(row_of(key_ref, s, h))
    qn = unit_rows(row_of(query_ref, s, h))
    bn = 1.0 / (1.0 + jnp.exp(-jnp.full((1, CH), gate_ref[s, h], F32)))
    meet = jnp.sum(kn * qn, axis=1, keepdims=True)
    out[:8, :] = jnp.concatenate(
        [kn, qn, row_of(value_ref, s, h), bn, bn * meet, jnp.zeros((3, CH), F32)], axis=0
    )
    diagonal = iota((ROWS, CH), 1) == iota((ROWS, CH), 0) + part * ROWS
    k_col = jnp.sum(jnp.where(diagonal, jnp.broadcast_to(kn, (ROWS, CH)), 0.0), axis=1, keepdims=True)
    out[8:, :] = bn * k_col


def halves_kernel(own, other, token, mine, theirs, scr, amap, gain):
    part = lax.axis_index("sp_0")
    odd = lax.rem(part, 2)
    scr[odd] = own[...]
    scr[1 - odd] = other[...]
    amap[...], gain[...] = after(
        (scr[0, :CH, :], scr[0, CH:, :]), (scr[1, :CH, :], scr[1, CH:, :])
    )

    @pl.when(part < 2)
    def _():
        mine[...] = gain[...]
        theirs[...] = gain[...]

    @pl.when(part >= 2)
    def _():
        through = dot3(token[:8, :], jnp.concatenate([amap[...], gain[...]], axis=1))
        for ref, owner in ((mine, part), (theirs, part - 2)):
            rows = pl.ds(pl.multiple_of(owner * ROWS, ROWS), ROWS)
            ref[:ROWS, :] = amap[rows, :]
            ref[ROWS : ROWS + 8, :] = through[:, :CH]
            ref[ROWS + 8 : 2 * ROWS + 8, :] = gain[rows, :]
            ref[2 * ROWS + 8 : 2 * ROWS + 16, :] = through[:, CH:]
            ref[2 * ROWS + 16 :, :] = jnp.zeros((CH - 2 * ROWS - 16, CH), F32)


def rows_kernel(mine, theirs, token, gain_ref, o0, o1, o2, o3, scr, wide):
    right = jnp.where(lax.axis_index("sp_0") < 2, 0, 1)
    scr[right] = mine[...]
    scr[1 - right] = theirs[...]
    final = dot3(scr[1, : ROWS + 8, :], scr[0]) + scr[1, ROWS + 8 : 2 * ROWS + 16, :]
    missing = token[2:3, :] - final[ROWS : ROWS + 1, :]
    wide[:ROWS, :] = final[:ROWS, :] + token[8:, :] * missing
    read = (final[ROWS + 1 : ROWS + 2, :] + token[4:5, :] * missing) / math.sqrt(CH)
    scale = lax.rsqrt(jnp.mean(read * read, axis=-1, keepdims=True) + 1e-06)
    read_rows = jnp.broadcast_to(read * scale * gain_ref[...], (8, CH))
    for k, o in zip(SHIFTS, (o0, o1, o2, o3)):
        y = lax.rem(lax.axis_index("sp_1") + k, 4)
        o[:8, :] = wide[pl.ds(pl.multiple_of(y * 8, 8), 8), :]
        o[8:, :] = read_rows


def finish_kernel(r0, r1, r2, r3, cache_ref, read_ref, scr):
    for k, ref in zip(SHIFTS, (r0, r1, r2, r3)):
        scr[lax.rem(lax.axis_index("sp_1") + 4 - k, 4)] = ref[...]
    for s in range(2):
        for h in range(2):
            cache_ref[s, h] = scr[2 * s + h, :8, :].astype(BF16)
        read_ref[s] = jnp.concatenate([scr[2 * s + h, 8:9, :] for h in range(2)], axis=0).astype(BF16)


def vmem(count):
    return [pl.BlockSpec(memory_space=pltpu.VMEM) for _ in range(count)]


def spread(arrays, axis):
    return [
        lax.ppermute(a, axis, [(i, (i + k) % 4) for i in range(4)]) if k else a
        for k, a in zip(SHIFTS, arrays)
    ]


def swap(array, axis, bit):
    return lax.ppermute(array, axis, [(i, i ^ bit) for i in range(4)])


def shards(
    tokens,
    key_matrix,
    value_matrix,
    gate_matrix,
    decay_matrix,
    gate_bias_offset,
    head_log_decay_rate,
    extra_log_decay,
    next_token_query,
    next_token_key,
    next_token_value,
    next_token_gate,
    readout_norm_gain,
):
    seqs, seg, width = tokens.shape
    cols = key_matrix.shape[1]
    tile = seg
    tiles = seqs * seg // tile
    chunks = seqs * seg // CH
    extra = jnp.transpose(extra_log_decay.reshape(chunks, CH, 2), (0, 2, 1))
    hbm = pl.BlockSpec(memory_space=pltpu.HBM)
    smem = pl.BlockSpec(memory_space=pltpu.SMEM)
    maps = pl.pallas_call(
        maps_kernel,
        out_shape=[jax.ShapeDtypeStruct((2 * CH, CH), F32)] * 4,
        in_specs=[hbm] * 8,
        out_specs=vmem(4),
        scratch_shapes=[
            pltpu.VMEM((tiles, tile, width), BF16),
            pltpu.VMEM((width, cols), BF16),
            pltpu.VMEM((width, cols), BF16),
            pltpu.VMEM((2 * gate_matrix.shape[1], width), BF16),
            pltpu.VMEM((chunks, 2, CH), F32),
            pltpu.SMEM(gate_bias_offset.shape, F32),
            pltpu.SMEM(head_log_decay_rate.shape, F32),
            pltpu.VMEM((seqs * seg, cols), BF16),
            pltpu.VMEM((seqs * seg, cols), BF16),
            pltpu.VMEM((4, 2 * CH, CH), F32),
            pltpu.SemaphoreType.DMA((11,)),
        ],
        compiler_params=pltpu.CompilerParams(vmem_limit_bytes=24 * 2**20),
        name="maps",
    )(
        *(
            pltpu.with_memory_space_constraint(a, pltpu.HBM)
            for a in (
                tokens,
                key_matrix,
                value_matrix,
                gate_matrix.T,
                decay_matrix.T,
                gate_bias_offset,
                head_log_decay_rate,
                extra,
            )
        )
    )
    small = pltpu.CompilerParams(vmem_limit_bytes=8 * 2**20)
    segment = pl.pallas_call(
        segments_kernel,
        out_shape=jax.ShapeDtypeStruct((2 * CH, CH), F32),
        in_specs=vmem(4),
        out_specs=vmem(1)[0],
        scratch_shapes=[pltpu.VMEM((4, 2 * CH, CH), F32)],
        compiler_params=small,
        name="segments",
    )(*spread(maps, "sp_1"))
    token = pl.pallas_call(
        token_kernel,
        out_shape=jax.ShapeDtypeStruct((8 + ROWS, CH), F32),
        in_specs=[*vmem(3), smem],
        out_specs=vmem(1)[0],
        compiler_params=small,
        name="token",
    )(next_token_query, next_token_key, next_token_value, next_token_gate)
    mine, theirs = pl.pallas_call(
        halves_kernel,
        out_shape=[jax.ShapeDtypeStruct((CH, CH), F32)] * 2,
        in_specs=vmem(3),
        out_specs=vmem(2),
        scratch_shapes=[
            pltpu.VMEM((2, 2 * CH, CH), F32),
            pltpu.VMEM((CH, CH), F32),
            pltpu.VMEM((CH, CH), F32),
        ],
        compiler_params=small,
        name="halves",
    )(segment, swap(segment, "sp_0", 1), token)
    rows = pl.pallas_call(
        rows_kernel,
        out_shape=[jax.ShapeDtypeStruct((16, CH), F32)] * 4,
        in_specs=vmem(4),
        out_specs=vmem(4),
        scratch_shapes=[pltpu.VMEM((2, CH, CH), F32), pltpu.VMEM((ROWS, CH), F32)],
        compiler_params=small,
        name="rows",
    )(mine, swap(theirs, "sp_0", 2), token, readout_norm_gain.reshape(1, CH))
    return pl.pallas_call(
        finish_kernel,
        out_shape=[
            jax.ShapeDtypeStruct((2, 2, 8, CH), BF16),
            jax.ShapeDtypeStruct((2, 2, CH), BF16),
        ],
        in_specs=vmem(4),
        out_specs=vmem(2),
        scratch_shapes=[pltpu.VMEM((4, 16, CH), F32)],
        compiler_params=small,
        name="finish",
    )(*spread(rows, "sp_1"))


def solution(mesh):
    finer = Mesh(
        mesh.devices.reshape(mesh.shape["gr"], 4, 4, mesh.shape["tp"]), ("gr", "sp_0", "sp_1", "tp")
    )
    in_specs = (
        P("gr", SP, None),
        P(None, "tp"),
        P(None, "tp"),
        P(),
        P(),
        P(),
        P(),
        P("gr", SP, "tp"),
        P("gr", "tp", None),
        P("gr", "tp", None),
        P("gr", "tp", None),
        P("gr", "tp"),
        P(),
    )
    out_specs = (P("gr", "tp", SP, None), P("gr", "tp", None))
    return jax.shard_map(
        shards, mesh=finer, in_specs=in_specs, out_specs=out_specs, check_vma=False
    )
```

```python
import math

import jax
import jax.numpy as jnp
from jax import lax
from jax.experimental import pallas as pl
from jax.experimental.pallas import tpu as pltpu
from jax.sharding import Mesh
from jax.sharding import PartitionSpec as P


SP = ("sp_0", "sp_1")
CH = 128
ROWS = 32
SHIFTS = (0, 2, 3, 1)
F32 = jnp.float32
BF16 = jnp.bfloat16
AB = (((1,), (0,)), ((), ()))
ABT = (((1,), (1,)), ((), ()))
ATB = (((0,), (0,)), ((), ()))


def dot1(a, b, dims=AB):
    return lax.dot_general(a.astype(BF16), b.astype(BF16), dims, preferred_element_type=F32)


def split(a):
    hi = a.astype(BF16)
    return hi, (a - hi.astype(F32)).astype(BF16)


def dot3(a, b, dims=AB):
    ah, al = split(a)
    bh, bl = split(b)
    return dot1(ah, bh, dims) + (dot1(ah, bl, dims) + dot1(al, bh, dims))


def iota(shape, dim):
    return lax.broadcasted_iota(jnp.int32, shape, dim)


def unit_rows(a):
    return a * lax.rsqrt(jnp.sum(a * a, axis=-1, keepdims=True) + 1e-06)


def silu(a):
    return a * (1.0 / (1.0 + jnp.exp(-a)))


def inverses_of(m_mats):
    row = iota((CH, CH), 0)
    col = iota((CH, CH), 1)
    eye = jnp.where(row == col, 1.0, 0.0)
    near = row // 16 == col // 16
    p1s = [jnp.where(near, -m, 0.0) for m in m_mats]
    invs = [eye + p for p in p1s]
    pows = [p.astype(BF16) for p in p1s]
    pows = [dot1(p, p).astype(BF16) for p in pows]
    for last in (False, False, True):
        if last:
            adds = [dot1(p, i) for p, i in zip(pows, invs)]
        else:
            both = [dot1(p, jnp.concatenate([p, i.astype(BF16)], axis=1)) for p, i in zip(pows, invs)]
            adds = [x[:, CH:] for x in both]
            pows = [x[:, :CH].astype(BF16) for x in both]
        invs = [i + x for i, x in zip(invs, adds)]
    for b in (16, 32, 64):
        lower = [slice(s + b, s + 2 * b) for s in range(0, CH, 2 * b)]

        def gather(rows_of):
            return jnp.concatenate([rows_of(r) for r in lower], axis=0)

        m_rows = [
            gather(lambda r: jnp.where(col[r, :] // b == (r.start // b - 1), m[r, :], 0.0))
            for m in m_mats
        ]
        t_rows = [gather(lambda r: i[r, :]) for i in invs]
        uppers = []
        for i in invs:
            pieces = []
            for r in lower:
                pieces += [i[r.start - b : r.start, :].astype(BF16), jnp.zeros((b, CH), BF16)]
            uppers.append(jnp.concatenate(pieces, axis=0))
        ys = [dot1(m, i).astype(BF16) for m, i in zip(m_rows, uppers)]
        spread_out = []
        for y in ys:
            pieces = []
            for g in range(len(lower)):
                pieces += [jnp.zeros((b, CH), BF16), y[g * b : (g + 1) * b, :]]
            spread_out.append(jnp.concatenate(pieces, axis=0))
        news = [t - dot1(t, y) for t, y in zip(t_rows, spread_out)]
        joined = []
        for i, new in zip(invs, news):
            pieces = []
            for g, r in enumerate(lower):
                pieces += [i[r.start - b : r.start, :], new[g * b : (g + 1) * b, :]]
            joined.append(jnp.concatenate(pieces, axis=0))
        invs = joined
    return invs


def joined(first, second, eye):
    c1, d1, b1 = first
    c2, d2, b2 = second
    moved = dot1(d2, jnp.concatenate([c1 * eye - d1, b1], axis=1))
    return c1 * c2, c2 * d1 + moved[:, :CH], c2 * b1 - moved[:, CH:] + b2


def sequence_maps(x, wk, wv, gatew, extra, rows, kbuf, vbuf, state, seq, arrivals, same, flip):
    here = lax.axis_index("sp_1")
    first_head = lax.axis_index("tp") * 2
    tile = x.shape[0]
    half = tile // 2
    chunks = tile // CH
    heads = gatew.shape[0] // 2
    pick = iota((heads, tile), 0)
    row = iota((CH, CH), 0)
    col = iota((CH, CH), 1)
    eye = jnp.where(row == col, 1.0, 0.0)
    upto = jnp.where(row <= col, 1.0, 0.0).astype(BF16)

    def times(i, weights, dims=AB):
        return lax.dot_general(
            x[i * half : (i + 1) * half], weights[...], dims, preferred_element_type=F32
        )

    def keys(i, kp):
        kp = silu(kp)
        for h in range(2):
            kbuf[h, i * half : (i + 1) * half, :] = unit_rows(kp[:, h * CH : (h + 1) * CH]).astype(BF16)

    def values(i, vp):
        vp = silu(vp).astype(BF16)
        for h in range(2):
            vbuf[h, i * half : (i + 1) * half, :] = vp[:, h * CH : (h + 1) * CH]

    arrivals[0]()
    g0 = times(0, gatew, ABT)
    k0 = times(0, wk)
    arrivals[1]()
    g1 = times(1, gatew, ABT)
    k1 = times(1, wk)
    keys(0, k0)
    arrivals[2]()
    bias, rate = rows[0:2, :], rows[2:4, :]
    gt = jnp.concatenate([jnp.transpose(g) for g in (g0, g1)], axis=1)
    picked = [
        jnp.sum(jnp.where(pick == first_head + h, part, 0.0), axis=0, keepdims=True)
        for part in (gt[:heads], gt[heads:])
        for h in range(2)
    ]
    gate = jnp.concatenate(picked[:2], axis=0)
    z = jnp.concatenate(picked[2:], axis=0)
    soft = jnp.maximum(z, 0.0) + jnp.log1p(jnp.exp(-jnp.abs(z)))
    steps, gates = [], []
    for n in range(chunks):
        lanes = slice(n * CH, (n + 1) * CH)
        steps.append(extra[seq * chunks + n] - rate * soft[:, lanes])
        gates.append(gate[:, lanes] + bias)
    step = jnp.concatenate(steps, axis=0)
    beta = 1.0 / (1.0 + jnp.exp(-jnp.concatenate(gates, axis=0)))
    hi = step.astype(BF16)
    rest = step - hi.astype(F32)
    mid = rest.astype(BF16)
    low = (rest - mid.astype(F32)).astype(BF16)
    cum = dot1(hi, upto) + (dot1(mid, upto) + dot1(low, upto))
    count = cum.shape[0]
    total = jnp.broadcast_to(cum[:, CH - 1 : CH], (count, CH))
    carry = jnp.exp(total)
    ecum = jnp.exp(cum)
    columns = jnp.transpose(
        jnp.concatenate(
            [cum + jnp.log(beta), jnp.exp(total - cum), jnp.zeros((CH - 2 * count, CH), F32)], axis=0
        )
    )
    keys(1, k1)
    v0 = times(0, wv)
    v1 = times(1, wv)
    values(0, v0)
    values(1, v1)
    items = [(n, h) for n in range(chunks) for h in range(2)]
    ks = [kbuf[h, n * CH : (n + 1) * CH, :] for n, h in items]
    grams = [lax.dot_general(k, k, ABT, preferred_element_type=F32) for k in ks]
    ms = [
        jnp.where(row > col, g * jnp.exp(columns[:, r : r + 1] - cum[r : r + 1, :]), 0.0)
        for r, g in enumerate(grams)
    ]
    invs = inverses_of(ms)
    us = [columns[:, count + r : count + r + 1] * inv * beta[r : r + 1, :] for r, inv in enumerate(invs)]
    pulls = [
        dot1(u * ecum[r : r + 1, :], k).astype(BF16) for r, (u, k) in enumerate(zip(us, ks))
    ]
    freshs = [
        dot1(u, vbuf[h, n * CH : (n + 1) * CH, :]).astype(BF16) for (n, h), u in zip(items, us)
    ]
    boths = [
        dot1(k, jnp.concatenate([pull, fresh], axis=1), ATB)
        for k, pull, fresh in zip(ks, pulls, freshs)
    ]
    maps = [
        [
            (carry[2 * n + h : 2 * n + h + 1, :], boths[2 * n + h][:, :CH], boths[2 * n + h][:, CH:])
            for n in range(chunks)
        ]
        for h in range(2)
    ]
    while len(maps[0]) > 1:
        maps = [[joined(m[i], m[i + 1], eye) for i in range(0, len(m), 2)] for m in maps]
    for h in range(2):
        c_row, drop, gain = maps[h][0]
        state[h, :CH, :] = c_row * eye - drop
        state[h, CH:, :] = gain
    parity = lax.rem(here, 2)
    same[...] = state[parity]
    flip[...] = state[1 - parity]


def far_kernel(
    x_hbm, wk_hbm, wv_hbm, gate_hbm, decay_hbm, bias_hbm, rate_hbm, extra_hbm,
    same, flip, x_kept, wk, wv, gatew, extra, rows,
    x, bias_ref, rate_ref, kbuf, vbuf, state, sems,
):
    first_head = lax.axis_index("tp") * 2
    own = lax.div(lax.axis_index("sp_1"), 2)
    half = x.shape[0] // 2
    heads = gate_hbm.shape[0]
    top, low = pl.ds(0, half), pl.ds(half, half)
    moves = [
        (gate_hbm, gatew.at[pl.ds(0, heads)]),
        (decay_hbm, gatew.at[pl.ds(heads, heads)]),
        (bias_hbm, bias_ref),
        (rate_hbm, rate_ref),
        (extra_hbm, extra),
        (x_hbm.at[1 - own, top], x.at[top]),
        (wk_hbm, wk),
        (x_hbm.at[1 - own, low], x.at[low]),
        (wv_hbm, wv),
        (x_hbm.at[own], x_kept),
    ]
    copies = [pltpu.make_async_copy(src, dst, sems.at[i]) for i, (src, dst) in enumerate(moves)]
    for c in copies:
        c.start()
    for c in copies[:5]:
        c.wait()
    odd = iota((2, CH), 0) == 1
    rows[0:2, :] = jnp.where(odd, bias_ref[first_head + 1], bias_ref[first_head])
    rows[2:4, :] = jnp.exp(jnp.where(odd, rate_ref[first_head + 1], rate_ref[first_head]))
    rows[4:, :] = jnp.zeros((4, CH), F32)

    def first():
        copies[5].wait()
        copies[6].wait()

    arrivals = (first, copies[7].wait, copies[8].wait)
    sequence_maps(
        x, wk, wv, gatew, extra, rows, kbuf, vbuf, state, 1 - own, arrivals, same, flip
    )
    copies[9].wait()


def near_kernel(x, wk, wv, gatew, extra, rows, same, flip, kbuf, vbuf, state):
    own = lax.div(lax.axis_index("sp_1"), 2)
    arrivals = (lambda: None,) * 3
    sequence_maps(x, wk, wv, gatew, extra, rows, kbuf, vbuf, state, own, arrivals, same, flip)


def after(first, second):
    both = dot3(second[0], jnp.concatenate(first, axis=1))
    return both[:, :CH], both[:, CH:] + second[1]


def segments_kernel(r0, r1, r2, r3, out, scr):
    here = lax.axis_index("sp_1")
    for k, ref in enumerate((r0, r1, r2, r3)):
        scr[jnp.bitwise_xor(here, k)] = ref[...]
    maps = [(scr[t, :CH, :], scr[t, CH:, :]) for t in range(4)]
    while len(maps) > 1:
        maps = [after(maps[i], maps[i + 1]) for i in range(0, len(maps), 2)]
    out[:CH, :], out[CH:, :] = maps[0]


def row_of(ref, s, h):
    two = ref[s].astype(F32)
    return jnp.sum(jnp.where(iota(two.shape, 0) == h, two, 0.0), axis=0, keepdims=True)


def token_kernel(query_ref, key_ref, value_ref, gate_ref, out):
    part = lax.axis_index("sp_0")
    pair = lax.axis_index("sp_1")
    s, h = lax.div(pair, 2), lax.rem(pair, 2)
    kn = unit_rows(row_of(key_ref, s, h))
    qn = unit_rows(row_of(query_ref, s, h))
    bn = 1.0 / (1.0 + jnp.exp(-jnp.full((1, CH), gate_ref[s, h], F32)))
    meet = jnp.sum(kn * qn, axis=1, keepdims=True)
    out[:8, :] = jnp.concatenate(
        [kn, qn, row_of(value_ref, s, h), bn, bn * meet, jnp.zeros((3, CH), F32)], axis=0
    )
    diagonal = iota((ROWS, CH), 1) == iota((ROWS, CH), 0) + part * ROWS
    k_col = jnp.sum(jnp.where(diagonal, jnp.broadcast_to(kn, (ROWS, CH)), 0.0), axis=1, keepdims=True)
    out[8:, :] = bn * k_col


def halves_kernel(own, other, token, mine, theirs, scr, amap, gain):
    part = lax.axis_index("sp_0")
    odd = lax.rem(part, 2)
    scr[odd] = own[...]
    scr[1 - odd] = other[...]
    amap[...], gain[...] = after(
        (scr[0, :CH, :], scr[0, CH:, :]), (scr[1, :CH, :], scr[1, CH:, :])
    )

    @pl.when(part < 2)
    def _():
        mine[...] = gain[...]
        theirs[...] = gain[...]

    @pl.when(part >= 2)
    def _():
        through = dot3(token[:8, :], jnp.concatenate([amap[...], gain[...]], axis=1))
        for ref, owner in ((mine, part), (theirs, part - 2)):
            rows = pl.ds(pl.multiple_of(owner * ROWS, ROWS), ROWS)
            ref[:ROWS, :] = amap[rows, :]
            ref[ROWS : ROWS + 8, :] = through[:, :CH]
            ref[ROWS + 8 : 2 * ROWS + 8, :] = gain[rows, :]
            ref[2 * ROWS + 8 : 2 * ROWS + 16, :] = through[:, CH:]
            ref[2 * ROWS + 16 :, :] = jnp.zeros((CH - 2 * ROWS - 16, CH), F32)


def rows_kernel(mine, theirs, token, gain_ref, o0, o1, o2, o3, scr, wide):
    right = jnp.where(lax.axis_index("sp_0") < 2, 0, 1)
    scr[right] = mine[...]
    scr[1 - right] = theirs[...]
    final = dot3(scr[1, : ROWS + 8, :], scr[0]) + scr[1, ROWS + 8 : 2 * ROWS + 16, :]
    missing = token[2:3, :] - final[ROWS : ROWS + 1, :]
    wide[:ROWS, :] = final[:ROWS, :] + token[8:, :] * missing
    read = (final[ROWS + 1 : ROWS + 2, :] + token[4:5, :] * missing) / math.sqrt(CH)
    scale = lax.rsqrt(jnp.mean(read * read, axis=-1, keepdims=True) + 1e-06)
    read_rows = jnp.broadcast_to(read * scale * gain_ref[...], (8, CH))
    for k, o in zip(SHIFTS, (o0, o1, o2, o3)):
        y = lax.rem(lax.axis_index("sp_1") + k, 4)
        o[:8, :] = wide[pl.ds(pl.multiple_of(y * 8, 8), 8), :]
        o[8:, :] = read_rows


def finish_kernel(r0, r1, r2, r3, cache_ref, read_ref, scr):
    for k, ref in zip(SHIFTS, (r0, r1, r2, r3)):
        scr[lax.rem(lax.axis_index("sp_1") + 4 - k, 4)] = ref[...]
    for s in range(2):
        for h in range(2):
            cache_ref[s, h] = scr[2 * s + h, :8, :].astype(BF16)
        read_ref[s] = jnp.concatenate([scr[2 * s + h, 8:9, :] for h in range(2)], axis=0).astype(BF16)


def vmem(count):
    return [pl.BlockSpec(memory_space=pltpu.VMEM) for _ in range(count)]


def spread(arrays, axis):
    return [
        lax.ppermute(a, axis, [(i, (i + k) % 4) for i in range(4)]) if k else a
        for k, a in zip(SHIFTS, arrays)
    ]


def swap(array, axis, bit):
    return lax.ppermute(array, axis, [(i, i ^ bit) for i in range(4)])


def shards(
    tokens,
    key_matrix,
    value_matrix,
    gate_matrix,
    decay_matrix,
    gate_bias_offset,
    head_log_decay_rate,
    extra_log_decay,
    next_token_query,
    next_token_key,
    next_token_value,
    next_token_gate,
    readout_norm_gain,
):
    seqs, seg, width = tokens.shape
    cols = key_matrix.shape[1]
    gate_count = gate_matrix.shape[1]
    chunks = seqs * seg // CH
    extra = jnp.transpose(extra_log_decay.reshape(chunks, CH, 2), (0, 2, 1))
    hbm = pl.BlockSpec(memory_space=pltpu.HBM)
    smem = pl.BlockSpec(memory_space=pltpu.SMEM)
    halved = [pltpu.VMEM((2, seg, CH), BF16)] * 2 + [pltpu.VMEM((2, 2 * CH, CH), F32)]
    far2, far3, *kept = pl.pallas_call(
        far_kernel,
        out_shape=[jax.ShapeDtypeStruct((2 * CH, CH), F32)] * 2
        + [
            jax.ShapeDtypeStruct((seg, width), BF16),
            jax.ShapeDtypeStruct((width, cols), BF16),
            jax.ShapeDtypeStruct((width, cols), BF16),
            jax.ShapeDtypeStruct((2 * gate_count, width), BF16),
            jax.ShapeDtypeStruct((chunks, 2, CH), F32),
            jax.ShapeDtypeStruct((8, CH), F32),
        ],
        in_specs=[hbm] * 8,
        out_specs=vmem(8),
        scratch_shapes=[
            pltpu.VMEM((seg, width), BF16),
            pltpu.SMEM(gate_bias_offset.shape, F32),
            pltpu.SMEM(head_log_decay_rate.shape, F32),
            *halved,
            pltpu.SemaphoreType.DMA((10,)),
        ],
        compiler_params=pltpu.CompilerParams(vmem_limit_bytes=24 * 2**20),
        name="far",
    )(
        *(
            pltpu.with_memory_space_constraint(a, pltpu.HBM)
            for a in (
                tokens,
                key_matrix,
                value_matrix,
                gate_matrix.T,
                decay_matrix.T,
                gate_bias_offset,
                head_log_decay_rate,
                extra,
            )
        )
    )
    from2 = swap(far2, "sp_1", 2)
    from3 = swap(far3, "sp_1", 3)
    near = pl.pallas_call(
        near_kernel,
        out_shape=[jax.ShapeDtypeStruct((2 * CH, CH), F32)] * 2,
        in_specs=vmem(6),
        out_specs=vmem(2),
        scratch_shapes=halved,
        compiler_params=pltpu.CompilerParams(vmem_limit_bytes=16 * 2**20),
        cost_estimate=pl.CostEstimate(flops=3 * 10**9, bytes_accessed=10**6, transcendentals=0),
        name="near",
    )
    mine, near1 = near(*kept)
    small = pltpu.CompilerParams(vmem_limit_bytes=8 * 2**20)
    segment = pl.pallas_call(
        segments_kernel,
        out_shape=jax.ShapeDtypeStruct((2 * CH, CH), F32),
        in_specs=vmem(4),
        out_specs=vmem(1)[0],
        scratch_shapes=[pltpu.VMEM((4, 2 * CH, CH), F32)],
        compiler_params=small,
        name="segments",
    )(mine, swap(near1, "sp_1", 1), from2, from3)
    token = pl.pallas_call(
        token_kernel,
        out_shape=jax.ShapeDtypeStruct((8 + ROWS, CH), F32),
        in_specs=[*vmem(3), smem],
        out_specs=vmem(1)[0],
        compiler_params=small,
        name="token",
    )(next_token_query, next_token_key, next_token_value, next_token_gate)
    mine, theirs = pl.pallas_call(
        halves_kernel,
        out_shape=[jax.ShapeDtypeStruct((CH, CH), F32)] * 2,
        in_specs=vmem(3),
        out_specs=vmem(2),
        scratch_shapes=[
            pltpu.VMEM((2, 2 * CH, CH), F32),
            pltpu.VMEM((CH, CH), F32),
            pltpu.VMEM((CH, CH), F32),
        ],
        compiler_params=small,
        name="halves",
    )(segment, swap(segment, "sp_0", 1), token)
    rows = pl.pallas_call(
        rows_kernel,
        out_shape=[jax.ShapeDtypeStruct((16, CH), F32)] * 4,
        in_specs=vmem(4),
        out_specs=vmem(4),
        scratch_shapes=[pltpu.VMEM((2, CH, CH), F32), pltpu.VMEM((ROWS, CH), F32)],
        compiler_params=small,
        name="rows",
    )(mine, swap(theirs, "sp_0", 2), token, readout_norm_gain.reshape(1, CH))
    return pl.pallas_call(
        finish_kernel,
        out_shape=[
            jax.ShapeDtypeStruct((2, 2, 8, CH), BF16),
            jax.ShapeDtypeStruct((2, 2, CH), BF16),
        ],
        in_specs=vmem(4),
        out_specs=vmem(2),
        scratch_shapes=[pltpu.VMEM((4, 16, CH), F32)],
        compiler_params=small,
        name="finish",
    )(*spread(rows, "sp_1"))


def solution(mesh):
    finer = Mesh(
        mesh.devices.reshape(mesh.shape["gr"], 4, 4, mesh.shape["tp"]), ("gr", "sp_0", "sp_1", "tp")
    )
    in_specs = (
        P("gr", SP, None),
        P(None, "tp"),
        P(None, "tp"),
        P(),
        P(),
        P(),
        P(),
        P("gr", SP, "tp"),
        P("gr", "tp", None),
        P("gr", "tp", None),
        P("gr", "tp", None),
        P("gr", "tp"),
        P(),
    )
    out_specs = (P("gr", "tp", SP, None), P("gr", "tp", None))
    return jax.shard_map(
        shards, mesh=finer, in_specs=in_specs, out_specs=out_specs, check_vma=False
    )
```

```python
import math

import jax
import jax.numpy as jnp
from jax import lax
from jax.experimental import pallas as pl
from jax.experimental.pallas import tpu as pltpu
from jax.sharding import Mesh
from jax.sharding import PartitionSpec as P


SP = ("sp_0", "sp_1")
CH = 128
ROWS = 32
SHIFTS = (0, 2, 3, 1)
F32 = jnp.float32
BF16 = jnp.bfloat16
AB = (((1,), (0,)), ((), ()))
ABT = (((1,), (1,)), ((), ()))
ATB = (((0,), (0,)), ((), ()))


def dot1(a, b, dims=AB):
    return lax.dot_general(a.astype(BF16), b.astype(BF16), dims, preferred_element_type=F32)


def split(a):
    hi = a.astype(BF16)
    return hi, (a - hi.astype(F32)).astype(BF16)


def dot3(a, b, dims=AB):
    ah, al = split(a)
    bh, bl = split(b)
    return dot1(ah, bh, dims) + (dot1(ah, bl, dims) + dot1(al, bh, dims))


def iota(shape, dim):
    return lax.broadcasted_iota(jnp.int32, shape, dim)


def unit_rows(a):
    return a * lax.rsqrt(jnp.sum(a * a, axis=-1, keepdims=True) + 1e-06)


def silu(a):
    return a * (1.0 / (1.0 + jnp.exp(-a)))


def inverses_of(m_mats):
    row = iota((CH, CH), 0)
    col = iota((CH, CH), 1)
    eye = jnp.where(row == col, 1.0, 0.0)
    near = row // 16 == col // 16
    p1s = [jnp.where(near, -m, 0.0) for m in m_mats]
    invs = [eye + p for p in p1s]
    pows = [p.astype(BF16) for p in p1s]
    pows = [dot1(p, p).astype(BF16) for p in pows]
    for last in (False, False, True):
        if last:
            adds = [dot1(p, i) for p, i in zip(pows, invs)]
        else:
            both = [dot1(p, jnp.concatenate([p, i.astype(BF16)], axis=1)) for p, i in zip(pows, invs)]
            adds = [x[:, CH:] for x in both]
            pows = [x[:, :CH].astype(BF16) for x in both]
        invs = [i + x for i, x in zip(invs, adds)]
    for b in (16, 32, 64):
        lower = [slice(s + b, s + 2 * b) for s in range(0, CH, 2 * b)]

        def gather(rows_of):
            return jnp.concatenate([rows_of(r) for r in lower], axis=0)

        m_rows = [
            gather(lambda r: jnp.where(col[r, :] // b == (r.start // b - 1), m[r, :], 0.0))
            for m in m_mats
        ]
        t_rows = [gather(lambda r: i[r, :]) for i in invs]
        uppers = []
        for i in invs:
            pieces = []
            for r in lower:
                pieces += [i[r.start - b : r.start, :].astype(BF16), jnp.zeros((b, CH), BF16)]
            uppers.append(jnp.concatenate(pieces, axis=0))
        ys = [dot1(m, i).astype(BF16) for m, i in zip(m_rows, uppers)]
        spread_out = []
        for y in ys:
            pieces = []
            for g in range(len(lower)):
                pieces += [jnp.zeros((b, CH), BF16), y[g * b : (g + 1) * b, :]]
            spread_out.append(jnp.concatenate(pieces, axis=0))
        news = [t - dot1(t, y) for t, y in zip(t_rows, spread_out)]
        joined = []
        for i, new in zip(invs, news):
            pieces = []
            for g, r in enumerate(lower):
                pieces += [i[r.start - b : r.start, :], new[g * b : (g + 1) * b, :]]
            joined.append(jnp.concatenate(pieces, axis=0))
        invs = joined
    return invs


def joined(first, second, eye):
    c1, d1, b1 = first
    c2, d2, b2 = second
    moved = dot1(d2, jnp.concatenate([c1 * eye - d1, b1], axis=1))
    return c1 * c2, c2 * d1 + moved[:, :CH], c2 * b1 - moved[:, CH:] + b2


def pair_maps(k_of, v_of, rows_of):
    row = iota((CH, CH), 0)
    col = iota((CH, CH), 1)
    eye = jnp.where(row == col, 1.0, 0.0)
    pairs = range(len(k_of))
    chunks = k_of[0].shape[0] // CH
    beta = [r[:chunks] for r in rows_of]
    cum = [r[chunks:] for r in rows_of]
    total = [jnp.broadcast_to(c[:, CH - 1 : CH], (chunks, CH)) for c in cum]
    carry = [jnp.exp(t) for t in total]
    ecum = [jnp.exp(c) for c in cum]
    columns = [
        jnp.transpose(
            jnp.concatenate(
                [c + jnp.log(b), jnp.exp(t - c), jnp.zeros((CH - 2 * chunks, CH), F32)], axis=0
            )
        )
        for b, c, t in zip(beta, cum, total)
    ]
    items = [(p, n) for p in pairs for n in range(chunks)]
    ks = [k_of[p][n * CH : (n + 1) * CH] for p, n in items]
    vs = [v_of[p][n * CH : (n + 1) * CH] for p, n in items]
    grams = [lax.dot_general(k, k, ABT, preferred_element_type=F32) for k in ks]
    ms = [
        jnp.where(row > col, g * jnp.exp(columns[p][:, n : n + 1] - cum[p][n : n + 1, :]), 0.0)
        for (p, n), g in zip(items, grams)
    ]
    invs = inverses_of(ms)
    us = [
        columns[p][:, chunks + n : chunks + n + 1] * inv * beta[p][n : n + 1, :]
        for (p, n), inv in zip(items, invs)
    ]
    pulls = [
        dot1(u * ecum[p][n : n + 1, :], k).astype(BF16) for (p, n), u, k in zip(items, us, ks)
    ]
    freshs = [dot1(u, v).astype(BF16) for u, v in zip(us, vs)]
    boths = [
        dot1(k, jnp.concatenate([pull, fresh], axis=1), ATB)
        for k, pull, fresh in zip(ks, pulls, freshs)
    ]
    maps = [[] for _ in pairs]
    for (p, n), both in zip(items, boths):
        maps[p].append((carry[p][n : n + 1, :], both[:, :CH], both[:, CH:]))
    while len(maps[0]) > 1:
        maps = [[joined(m[i], m[i + 1], eye) for i in range(0, len(m), 2)] for m in maps]
    return [(c_row * eye - drop, gain) for ((c_row, drop, gain),) in maps]


def far_kernel(
    x_hbm, wk_hbm, wv_hbm, gate_hbm, decay_hbm, bias_hbm, rate_hbm, extra_hbm,
    o2, o3, o1, k_own, v_own, rows_own,
    xbuf, wkbuf, wvbuf, gatew, extra, bias_ref, rate_ref, kbuf, vbuf, rows, sems,
):
    tiles, tile, _ = xbuf.shape
    half = tile // 2
    first_head = lax.axis_index("tp") * 2
    here = lax.axis_index("sp_1")
    chunks = tile // CH
    heads = gate_hbm.shape[0]
    moves = [
        (gate_hbm, gatew.at[pl.ds(0, heads)]),
        (decay_hbm, gatew.at[pl.ds(heads, heads)]),
        (bias_hbm, bias_ref),
        (rate_hbm, rate_ref),
        (extra_hbm, extra),
    ]
    small = len(moves)
    for t in range(tiles):
        for i in range(2):
            part = pl.ds(i * half, half)
            moves.append((x_hbm.at[t, part], xbuf.at[t, part]))
            if t == 0:
                moves.append(((wk_hbm, wkbuf), (wv_hbm, wvbuf))[i])
    copies = [pltpu.make_async_copy(src, dst, sems.at[i]) for i, (src, dst) in enumerate(moves)]
    for c in copies:
        c.start()
    for c in copies[:small]:
        c.wait()
    x00, wk, x01, wv, x10, x11 = copies[small:]
    pick = iota((heads, tile), 0)
    odd = iota((2, CH), 0) == 1
    bias = jnp.where(odd, bias_ref[first_head + 1], bias_ref[first_head])
    rate = jnp.exp(jnp.where(odd, rate_ref[first_head + 1], rate_ref[first_head]))
    upto = jnp.where(iota((CH, CH), 0) <= iota((CH, CH), 1), 1.0, 0.0).astype(BF16)

    def times(t, i, weights, dims=AB):
        x = xbuf[t, i * half : (i + 1) * half]
        return lax.dot_general(x, weights[...], dims, preferred_element_type=F32)

    def keys(t, i, kp):
        kp = silu(kp)
        for h in range(2):
            part = unit_rows(kp[:, h * CH : (h + 1) * CH])
            kbuf[2 * t + h, i * half : (i + 1) * half, :] = part.astype(BF16)

    def values(t, i, vp):
        vp = silu(vp).astype(BF16)
        for h in range(2):
            vbuf[2 * t + h, i * half : (i + 1) * half, :] = vp[:, h * CH : (h + 1) * CH]

    def scalars(t, gts):
        gt = jnp.concatenate([jnp.transpose(g) for g in gts], axis=1)
        picked = [
            jnp.sum(jnp.where(pick == first_head + h, part, 0.0), axis=0, keepdims=True)
            for part in (gt[:heads], gt[heads:])
            for h in range(2)
        ]
        gate = jnp.concatenate(picked[:2], axis=0)
        z = jnp.concatenate(picked[2:], axis=0)
        soft = jnp.maximum(z, 0.0) + jnp.log1p(jnp.exp(-jnp.abs(z)))
        steps, gates = [], []
        for n in range(chunks):
            lanes = slice(n * CH, (n + 1) * CH)
            steps.append(extra[t * chunks + n] - rate * soft[:, lanes])
            gates.append(gate[:, lanes] + bias)
        step = jnp.concatenate(steps, axis=0)
        beta = 1.0 / (1.0 + jnp.exp(-jnp.concatenate(gates, axis=0)))
        hi = step.astype(BF16)
        rest = step - hi.astype(F32)
        mid = rest.astype(BF16)
        low = (rest - mid.astype(F32)).astype(BF16)
        cum = dot1(hi, upto) + (dot1(mid, upto) + dot1(low, upto))
        for h in range(2):
            for n in range(chunks):
                r = 2 * n + h
                rows[2 * t + h, n : n + 1, :] = beta[r : r + 1, :]
                rows[2 * t + h, chunks + n : chunks + n + 1, :] = cum[r : r + 1, :]

    x00.wait()
    wk.wait()
    g00 = times(0, 0, gatew, ABT)
    k00 = times(0, 0, wkbuf)
    x01.wait()
    g01 = times(0, 1, gatew, ABT)
    k01 = times(0, 1, wkbuf)
    keys(0, 0, k00)
    wv.wait()
    v00 = times(0, 0, wvbuf)
    v01 = times(0, 1, wvbuf)
    keys(0, 1, k01)
    x10.wait()
    x11.wait()
    g10 = times(1, 0, gatew, ABT)
    k10 = times(1, 0, wkbuf)
    scalars(0, (g00, g01))
    g11 = times(1, 1, gatew, ABT)
    k11 = times(1, 1, wkbuf)
    values(0, 0, v00)
    values(0, 1, v01)
    scalars(1, (g10, g11))
    keys(1, 0, k10)
    v10 = times(1, 0, wvbuf)
    v11 = times(1, 1, wvbuf)
    keys(1, 1, k11)
    values(1, 0, v10)
    values(1, 1, v11)
    others = [jnp.bitwise_xor(here, bit) for bit in (2, 3, 1)]
    maps = pair_maps([kbuf[p] for p in others], [vbuf[p] for p in others], [rows[p] for p in others])
    for o, (amap, gain) in zip((o2, o3, o1), maps):
        o[:CH, :] = amap
        o[CH:, :] = gain
    k_own[...] = kbuf[here]
    v_own[...] = vbuf[here]
    rows_own[...] = rows[here]


def own_kernel(k_own, v_own, rows_own, out):
    out[:CH, :], out[CH:, :] = pair_maps([k_own[...]], [v_own[...]], [rows_own[...]])[0]


def after(first, second):
    both = dot3(second[0], jnp.concatenate(first, axis=1))
    return both[:, :CH], both[:, CH:] + second[1]


def segments_kernel(r0, r1, r2, r3, out, scr):
    here = lax.axis_index("sp_1")
    for k, ref in enumerate((r0, r1, r2, r3)):
        scr[jnp.bitwise_xor(here, k)] = ref[...]
    maps = [(scr[t, :CH, :], scr[t, CH:, :]) for t in range(4)]
    while len(maps) > 1:
        maps = [after(maps[i], maps[i + 1]) for i in range(0, len(maps), 2)]
    out[:CH, :], out[CH:, :] = maps[0]


def row_of(ref, s, h):
    two = ref[s].astype(F32)
    return jnp.sum(jnp.where(iota(two.shape, 0) == h, two, 0.0), axis=0, keepdims=True)


def token_kernel(query_ref, key_ref, value_ref, gate_ref, out):
    part = lax.axis_index("sp_0")
    pair = lax.axis_index("sp_1")
    s, h = lax.div(pair, 2), lax.rem(pair, 2)
    kn = unit_rows(row_of(key_ref, s, h))
    qn = unit_rows(row_of(query_ref, s, h))
    bn = 1.0 / (1.0 + jnp.exp(-jnp.full((1, CH), gate_ref[s, h], F32)))
    meet = jnp.sum(kn * qn, axis=1, keepdims=True)
    out[:8, :] = jnp.concatenate(
        [kn, qn, row_of(value_ref, s, h), bn, bn * meet, jnp.zeros((3, CH), F32)], axis=0
    )
    diagonal = iota((ROWS, CH), 1) == iota((ROWS, CH), 0) + part * ROWS
    k_col = jnp.sum(jnp.where(diagonal, jnp.broadcast_to(kn, (ROWS, CH)), 0.0), axis=1, keepdims=True)
    out[8:, :] = bn * k_col


def halves_kernel(own, other, token, mine, theirs, scr, amap, gain):
    part = lax.axis_index("sp_0")
    odd = lax.rem(part, 2)
    scr[odd] = own[...]
    scr[1 - odd] = other[...]
    amap[...], gain[...] = after(
        (scr[0, :CH, :], scr[0, CH:, :]), (scr[1, :CH, :], scr[1, CH:, :])
    )

    @pl.when(part < 2)
    def _():
        mine[...] = gain[...]
        theirs[...] = gain[...]

    @pl.when(part >= 2)
    def _():
        through = dot3(token[:8, :], jnp.concatenate([amap[...], gain[...]], axis=1))
        for ref, owner in ((mine, part), (theirs, part - 2)):
            rows = pl.ds(pl.multiple_of(owner * ROWS, ROWS), ROWS)
            ref[:ROWS, :] = amap[rows, :]
            ref[ROWS : ROWS + 8, :] = through[:, :CH]
            ref[ROWS + 8 : 2 * ROWS + 8, :] = gain[rows, :]
            ref[2 * ROWS + 8 : 2 * ROWS + 16, :] = through[:, CH:]
            ref[2 * ROWS + 16 :, :] = jnp.zeros((CH - 2 * ROWS - 16, CH), F32)


def rows_kernel(mine, theirs, token, gain_ref, o0, o1, o2, o3, scr, wide):
    right = jnp.where(lax.axis_index("sp_0") < 2, 0, 1)
    scr[right] = mine[...]
    scr[1 - right] = theirs[...]
    final = dot3(scr[1, : ROWS + 8, :], scr[0]) + scr[1, ROWS + 8 : 2 * ROWS + 16, :]
    missing = token[2:3, :] - final[ROWS : ROWS + 1, :]
    wide[:ROWS, :] = final[:ROWS, :] + token[8:, :] * missing
    read = (final[ROWS + 1 : ROWS + 2, :] + token[4:5, :] * missing) / math.sqrt(CH)
    scale = lax.rsqrt(jnp.mean(read * read, axis=-1, keepdims=True) + 1e-06)
    read_rows = jnp.broadcast_to(read * scale * gain_ref[...], (8, CH))
    for k, o in zip(SHIFTS, (o0, o1, o2, o3)):
        y = lax.rem(lax.axis_index("sp_1") + k, 4)
        o[:8, :] = wide[pl.ds(pl.multiple_of(y * 8, 8), 8), :]
        o[8:, :] = read_rows


def finish_kernel(r0, r1, r2, r3, cache_ref, read_ref, scr):
    for k, ref in zip(SHIFTS, (r0, r1, r2, r3)):
        scr[lax.rem(lax.axis_index("sp_1") + 4 - k, 4)] = ref[...]
    for s in range(2):
        for h in range(2):
            cache_ref[s, h] = scr[2 * s + h, :8, :].astype(BF16)
        read_ref[s] = jnp.concatenate([scr[2 * s + h, 8:9, :] for h in range(2)], axis=0).astype(BF16)


def vmem(count):
    return [pl.BlockSpec(memory_space=pltpu.VMEM) for _ in range(count)]


def spread(arrays, axis):
    return [
        lax.ppermute(a, axis, [(i, (i + k) % 4) for i in range(4)]) if k else a
        for k, a in zip(SHIFTS, arrays)
    ]


def swap(array, axis, bit):
    return lax.ppermute(array, axis, [(i, i ^ bit) for i in range(4)])


def shards(
    tokens,
    key_matrix,
    value_matrix,
    gate_matrix,
    decay_matrix,
    gate_bias_offset,
    head_log_decay_rate,
    extra_log_decay,
    next_token_query,
    next_token_key,
    next_token_value,
    next_token_gate,
    readout_norm_gain,
):
    seqs, seg, width = tokens.shape
    cols = key_matrix.shape[1]
    gate_count = gate_matrix.shape[1]
    chunks = seqs * seg // CH
    extra = jnp.transpose(extra_log_decay.reshape(chunks, CH, 2), (0, 2, 1))
    hbm = pl.BlockSpec(memory_space=pltpu.HBM)
    smem = pl.BlockSpec(memory_space=pltpu.SMEM)
    tiles = seqs
    far2, far3, far1, *kept = pl.pallas_call(
        far_kernel,
        out_shape=[jax.ShapeDtypeStruct((2 * CH, CH), F32)] * 3
        + [jax.ShapeDtypeStruct((seg, CH), BF16)] * 2
        + [jax.ShapeDtypeStruct((2 * seg // CH, CH), F32)],
        in_specs=[hbm] * 8,
        out_specs=vmem(6),
        scratch_shapes=[
            pltpu.VMEM((tiles, seg, width), BF16),
            pltpu.VMEM((width, cols), BF16),
            pltpu.VMEM((width, cols), BF16),
            pltpu.VMEM((2 * gate_count, width), BF16),
            pltpu.VMEM((chunks, 2, CH), F32),
            pltpu.SMEM(gate_bias_offset.shape, F32),
            pltpu.SMEM(head_log_decay_rate.shape, F32),
            pltpu.VMEM((4, seg, CH), BF16),
            pltpu.VMEM((4, seg, CH), BF16),
            pltpu.VMEM((4, 2 * seg // CH, CH), F32),
            pltpu.SemaphoreType.DMA((11,)),
        ],
        compiler_params=pltpu.CompilerParams(vmem_limit_bytes=24 * 2**20),
        name="far",
    )(
        *(
            pltpu.with_memory_space_constraint(a, pltpu.HBM)
            for a in (
                tokens,
                key_matrix,
                value_matrix,
                gate_matrix.T,
                decay_matrix.T,
                gate_bias_offset,
                head_log_decay_rate,
                extra,
            )
        )
    )
    arrived = []
    for array, bit in ((far2, 2), (far3, 3), (far1, 1)):
        arrived.append(swap(array, "sp_1", bit))
    near = pl.pallas_call(
        own_kernel,
        out_shape=jax.ShapeDtypeStruct((2 * CH, CH), F32),
        in_specs=vmem(3),
        out_specs=vmem(1)[0],
        compiler_params=pltpu.CompilerParams(vmem_limit_bytes=16 * 2**20),
        cost_estimate=pl.CostEstimate(flops=10**9, bytes_accessed=10**6, transcendentals=0),
        name="near",
    )
    mine = near(*kept)
    small = pltpu.CompilerParams(vmem_limit_bytes=8 * 2**20)
    segment = pl.pallas_call(
        segments_kernel,
        out_shape=jax.ShapeDtypeStruct((2 * CH, CH), F32),
        in_specs=vmem(4),
        out_specs=vmem(1)[0],
        scratch_shapes=[pltpu.VMEM((4, 2 * CH, CH), F32)],
        compiler_params=small,
        name="segments",
    )(mine, arrived[2], arrived[0], arrived[1])
    token = pl.pallas_call(
        token_kernel,
        out_shape=jax.ShapeDtypeStruct((8 + ROWS, CH), F32),
        in_specs=[*vmem(3), smem],
        out_specs=vmem(1)[0],
        compiler_params=small,
        name="token",
    )(next_token_query, next_token_key, next_token_value, next_token_gate)
    mine, theirs = pl.pallas_call(
        halves_kernel,
        out_shape=[jax.ShapeDtypeStruct((CH, CH), F32)] * 2,
        in_specs=vmem(3),
        out_specs=vmem(2),
        scratch_shapes=[
            pltpu.VMEM((2, 2 * CH, CH), F32),
            pltpu.VMEM((CH, CH), F32),
            pltpu.VMEM((CH, CH), F32),
        ],
        compiler_params=small,
        name="halves",
    )(segment, swap(segment, "sp_0", 1), token)
    rows = pl.pallas_call(
        rows_kernel,
        out_shape=[jax.ShapeDtypeStruct((16, CH), F32)] * 4,
        in_specs=vmem(4),
        out_specs=vmem(4),
        scratch_shapes=[pltpu.VMEM((2, CH, CH), F32), pltpu.VMEM((ROWS, CH), F32)],
        compiler_params=small,
        name="rows",
    )(mine, swap(theirs, "sp_0", 2), token, readout_norm_gain.reshape(1, CH))
    return pl.pallas_call(
        finish_kernel,
        out_shape=[
            jax.ShapeDtypeStruct((2, 2, 8, CH), BF16),
            jax.ShapeDtypeStruct((2, 2, CH), BF16),
        ],
        in_specs=vmem(4),
        out_specs=vmem(2),
        scratch_shapes=[pltpu.VMEM((4, 16, CH), F32)],
        compiler_params=small,
        name="finish",
    )(*spread(rows, "sp_1"))


def solution(mesh):
    finer = Mesh(
        mesh.devices.reshape(mesh.shape["gr"], 4, 4, mesh.shape["tp"]), ("gr", "sp_0", "sp_1", "tp")
    )
    in_specs = (
        P("gr", SP, None),
        P(None, "tp"),
        P(None, "tp"),
        P(),
        P(),
        P(),
        P(),
        P("gr", SP, "tp"),
        P("gr", "tp", None),
        P("gr", "tp", None),
        P("gr", "tp", None),
        P("gr", "tp"),
        P(),
    )
    out_specs = (P("gr", "tp", SP, None), P("gr", "tp", None))
    return jax.shard_map(
        shards, mesh=finer, in_specs=in_specs, out_specs=out_specs, check_vma=False
    )
```

```python
import math

import jax
import jax.numpy as jnp
from jax import lax
from jax.experimental import pallas as pl
from jax.experimental.pallas import tpu as pltpu
from jax.sharding import Mesh
from jax.sharding import PartitionSpec as P


SP = ("sp_0", "sp_1")
CH = 128
ROWS = 32
SHIFTS = (0, 2, 1, 3)
F32 = jnp.float32
BF16 = jnp.bfloat16
AB = (((1,), (0,)), ((), ()))
ABT = (((1,), (1,)), ((), ()))
ATB = (((0,), (0,)), ((), ()))


def dot1(a, b, dims=AB):
    return lax.dot_general(a.astype(BF16), b.astype(BF16), dims, preferred_element_type=F32)


def split(a):
    hi = a.astype(BF16)
    return hi, (a - hi.astype(F32)).astype(BF16)


def dot3(a, b, dims=AB):
    ah, al = split(a)
    bh, bl = split(b)
    return dot1(ah, bh, dims) + (dot1(ah, bl, dims) + dot1(al, bh, dims))


def iota(shape, dim):
    return lax.broadcasted_iota(jnp.int32, shape, dim)


def unit_rows(a):
    return a * lax.rsqrt(jnp.sum(a * a, axis=-1, keepdims=True) + 1e-06)


def silu(a):
    return a * (1.0 / (1.0 + jnp.exp(-a)))


def inverses_of(m_mats, fillers=()):
    row = iota((CH, CH), 0)
    col = iota((CH, CH), 1)
    eye = jnp.where(row == col, 1.0, 0.0)
    near = row // 16 == col // 16
    p1s = [jnp.where(near, -m, 0.0) for m in m_mats]
    invs = [eye + p for p in p1s]
    pows = [p.astype(BF16) for p in p1s]
    fillers = dict(fillers)

    def fill(step):
        if step in fillers:
            fillers[step]()

    fill(0)
    pows = [dot1(p, p).astype(BF16) for p in pows]
    fill(1)
    for step, last in enumerate((False, False, True)):
        if last:
            adds = [dot1(p, i) for p, i in zip(pows, invs)]
        else:
            both = [dot1(p, jnp.concatenate([p, i.astype(BF16)], axis=1)) for p, i in zip(pows, invs)]
            adds = [x[:, CH:] for x in both]
            pows = [x[:, :CH].astype(BF16) for x in both]
        invs = [i + x for i, x in zip(invs, adds)]
        fill(2 + step)
    for step, b in enumerate((16, 32, 64)):
        lower = [slice(s + b, s + 2 * b) for s in range(0, CH, 2 * b)]

        def gather(rows_of):
            return jnp.concatenate([rows_of(r) for r in lower], axis=0)

        m_rows = [
            gather(lambda r: jnp.where(col[r, :] // b == (r.start // b - 1), m[r, :], 0.0))
            for m in m_mats
        ]
        t_rows = [gather(lambda r: i[r, :]) for i in invs]
        uppers = []
        for i in invs:
            pieces = []
            for r in lower:
                pieces += [i[r.start - b : r.start, :].astype(BF16), jnp.zeros((b, CH), BF16)]
            uppers.append(jnp.concatenate(pieces, axis=0))
        ys = [dot1(m, i).astype(BF16) for m, i in zip(m_rows, uppers)]
        spread_out = []
        for y in ys:
            pieces = []
            for g in range(len(lower)):
                pieces += [jnp.zeros((b, CH), BF16), y[g * b : (g + 1) * b, :]]
            spread_out.append(jnp.concatenate(pieces, axis=0))
        fill(5 + 2 * step)
        news = [t - dot1(t, y) for t, y in zip(t_rows, spread_out)]
        joined = []
        for i, new in zip(invs, news):
            pieces = []
            for g, r in enumerate(lower):
                pieces += [i[r.start - b : r.start, :], new[g * b : (g + 1) * b, :]]
            joined.append(jnp.concatenate(pieces, axis=0))
        invs = joined
        fill(6 + 2 * step)
    return invs


def joined(first, second, eye):
    c1, d1, b1 = first
    c2, d2, b2 = second
    moved = dot1(d2, jnp.concatenate([c1 * eye - d1, b1], axis=1))
    return c1 * c2, c2 * d1 + moved[:, :CH], c2 * b1 - moved[:, CH:] + b2


def sequence_maps(x, wk, wv, gatew, extra, rows, kbuf, vbuf, state, seq, arrivals, same, flip):
    here = lax.axis_index("sp_1")
    first_head = lax.axis_index("tp") * 2
    tile = x.shape[0]
    half = tile // 2
    chunks = tile // CH
    heads = gatew.shape[0] // 2
    pick = iota((heads, tile), 0)
    row = iota((CH, CH), 0)
    col = iota((CH, CH), 1)
    eye = jnp.where(row == col, 1.0, 0.0)
    upto = jnp.where(row <= col, 1.0, 0.0).astype(BF16)

    def times(i, weights, dims=AB):
        return lax.dot_general(
            x[i * half : (i + 1) * half], weights[...], dims, preferred_element_type=F32
        )

    def keys(i, kp):
        kp = silu(kp)
        for h in range(2):
            kbuf[h, i * half : (i + 1) * half, :] = unit_rows(kp[:, h * CH : (h + 1) * CH]).astype(BF16)

    def values(i, vp):
        vp = silu(vp).astype(BF16)
        for h in range(2):
            vbuf[h, i * half : (i + 1) * half, :] = vp[:, h * CH : (h + 1) * CH]

    arrivals[0]()
    g0 = times(0, gatew, ABT)
    k0 = times(0, wk)
    arrivals[1]()
    g1 = times(1, gatew, ABT)
    k1 = times(1, wk)
    keys(0, k0)
    arrivals[2]()
    bias, rate = rows[0:2, :], rows[2:4, :]
    gt = jnp.concatenate([jnp.transpose(g) for g in (g0, g1)], axis=1)
    picked = [
        jnp.sum(jnp.where(pick == first_head + h, part, 0.0), axis=0, keepdims=True)
        for part in (gt[:heads], gt[heads:])
        for h in range(2)
    ]
    gate = jnp.concatenate(picked[:2], axis=0)
    z = jnp.concatenate(picked[2:], axis=0)
    soft = jnp.maximum(z, 0.0) + jnp.log1p(jnp.exp(-jnp.abs(z)))
    steps, gates = [], []
    for n in range(chunks):
        lanes = slice(n * CH, (n + 1) * CH)
        steps.append(extra[seq * chunks + n] - rate * soft[:, lanes])
        gates.append(gate[:, lanes] + bias)
    step = jnp.concatenate(steps, axis=0)
    beta = 1.0 / (1.0 + jnp.exp(-jnp.concatenate(gates, axis=0)))
    hi = step.astype(BF16)
    rest = step - hi.astype(F32)
    mid = rest.astype(BF16)
    low = (rest - mid.astype(F32)).astype(BF16)
    cum = dot1(hi, upto) + (dot1(mid, upto) + dot1(low, upto))
    count = cum.shape[0]
    total = jnp.broadcast_to(cum[:, CH - 1 : CH], (count, CH))
    carry = jnp.exp(total)
    ecum = jnp.exp(cum)
    columns = jnp.transpose(
        jnp.concatenate(
            [cum + jnp.log(beta), jnp.exp(total - cum), jnp.zeros((CH - 2 * count, CH), F32)], axis=0
        )
    )
    keys(1, k1)
    items = [(n, h) for n in range(chunks) for h in range(2)]
    ks = [kbuf[h, n * CH : (n + 1) * CH, :] for n, h in items]
    grams = [lax.dot_general(k, k, ABT, preferred_element_type=F32) for k in ks]
    ms = [
        jnp.where(row > col, g * jnp.exp(columns[:, r : r + 1] - cum[r : r + 1, :]), 0.0)
        for r, g in enumerate(grams)
    ]
    invs = inverses_of(
        ms, ((3, lambda: values(0, times(0, wv))), (7, lambda: values(1, times(1, wv))))
    )
    us = [columns[:, count + r : count + r + 1] * inv * beta[r : r + 1, :] for r, inv in enumerate(invs)]
    pulls = [
        dot1(u * ecum[r : r + 1, :], k).astype(BF16) for r, (u, k) in enumerate(zip(us, ks))
    ]
    freshs = [
        dot1(u, vbuf[h, n * CH : (n + 1) * CH, :]).astype(BF16) for (n, h), u in zip(items, us)
    ]
    boths = [
        dot1(k, jnp.concatenate([pull, fresh], axis=1), ATB)
        for k, pull, fresh in zip(ks, pulls, freshs)
    ]
    maps = [
        [
            (carry[2 * n + h : 2 * n + h + 1, :], boths[2 * n + h][:, :CH], boths[2 * n + h][:, CH:])
            for n in range(chunks)
        ]
        for h in range(2)
    ]
    while len(maps[0]) > 1:
        maps = [[joined(m[i], m[i + 1], eye) for i in range(0, len(m), 2)] for m in maps]
    for h in range(2):
        c_row, drop, gain = maps[h][0]
        state[h, :CH, :] = c_row * eye - drop
        state[h, CH:, :] = gain
    parity = lax.rem(here, 2)
    same[...] = state[parity]
    flip[...] = state[1 - parity]


def far_kernel(
    x_hbm, wk_hbm, wv_hbm, gate_hbm, decay_hbm, bias_hbm, rate_hbm, extra_hbm,
    same, flip, x_kept, wk, wv, gatew, extra, rows,
    x, bias_ref, rate_ref, kbuf, vbuf, state, sems,
):
    first_head = lax.axis_index("tp") * 2
    own = lax.div(lax.axis_index("sp_1"), 2)
    half = x.shape[0] // 2
    heads = gate_hbm.shape[0]
    top, low = pl.ds(0, half), pl.ds(half, half)
    moves = [
        (gate_hbm, gatew.at[pl.ds(0, heads)]),
        (decay_hbm, gatew.at[pl.ds(heads, heads)]),
        (bias_hbm, bias_ref),
        (rate_hbm, rate_ref),
        (extra_hbm, extra),
        (x_hbm.at[1 - own, top], x.at[top]),
        (wk_hbm, wk),
        (x_hbm.at[1 - own, low], x.at[low]),
        (wv_hbm, wv),
        (x_hbm.at[own], x_kept),
    ]
    copies = [pltpu.make_async_copy(src, dst, sems.at[i]) for i, (src, dst) in enumerate(moves)]
    for c in copies:
        c.start()
    for c in copies[:5]:
        c.wait()
    odd = iota((2, CH), 0) == 1
    rows[0:2, :] = jnp.where(odd, bias_ref[first_head + 1], bias_ref[first_head])
    rows[2:4, :] = jnp.exp(jnp.where(odd, rate_ref[first_head + 1], rate_ref[first_head]))
    rows[4:, :] = jnp.zeros((4, CH), F32)

    def first():
        copies[5].wait()
        copies[6].wait()

    arrivals = (first, copies[7].wait, copies[8].wait)
    sequence_maps(
        x, wk, wv, gatew, extra, rows, kbuf, vbuf, state, 1 - own, arrivals, same, flip
    )
    copies[9].wait()


def near_kernel(x, wk, wv, gatew, extra, rows, same, flip, kbuf, vbuf, state):
    own = lax.div(lax.axis_index("sp_1"), 2)
    arrivals = (lambda: None,) * 3
    sequence_maps(x, wk, wv, gatew, extra, rows, kbuf, vbuf, state, own, arrivals, same, flip)


def after(first, second):
    both = dot3(second[0], jnp.concatenate(first, axis=1))
    return both[:, :CH], both[:, CH:] + second[1]


def segments_kernel(r0, r1, r2, r3, out, scr):
    here = lax.axis_index("sp_1")
    for k, ref in enumerate((r0, r1, r2, r3)):
        scr[jnp.bitwise_xor(here, k)] = ref[...]
    maps = [(scr[t, :CH, :], scr[t, CH:, :]) for t in range(4)]
    while len(maps) > 1:
        maps = [after(maps[i], maps[i + 1]) for i in range(0, len(maps), 2)]
    out[:CH, :], out[CH:, :] = maps[0]


def row_of(ref, s, h):
    two = ref[s].astype(F32)
    return jnp.sum(jnp.where(iota(two.shape, 0) == h, two, 0.0), axis=0, keepdims=True)


def token_kernel(query_ref, key_ref, value_ref, gate_ref, out):
    part = lax.axis_index("sp_0")
    pair = lax.axis_index("sp_1")
    s, h = lax.div(pair, 2), lax.rem(pair, 2)
    kn = unit_rows(row_of(key_ref, s, h))
    qn = unit_rows(row_of(query_ref, s, h))
    bn = 1.0 / (1.0 + jnp.exp(-jnp.full((1, CH), gate_ref[s, h], F32)))
    meet = jnp.sum(kn * qn, axis=1, keepdims=True)
    out[:8, :] = jnp.concatenate(
        [kn, qn, row_of(value_ref, s, h), bn, bn * meet, jnp.zeros((3, CH), F32)], axis=0
    )
    diagonal = iota((ROWS, CH), 1) == iota((ROWS, CH), 0) + part * ROWS
    k_col = jnp.sum(jnp.where(diagonal, jnp.broadcast_to(kn, (ROWS, CH)), 0.0), axis=1, keepdims=True)
    out[8:, :] = bn * k_col


def halves_kernel(own, other, token, mine, theirs, scr, amap, gain):
    part = lax.axis_index("sp_0")
    odd = lax.rem(part, 2)
    scr[odd] = own[...]
    scr[1 - odd] = other[...]
    amap[...], gain[...] = after(
        (scr[0, :CH, :], scr[0, CH:, :]), (scr[1, :CH, :], scr[1, CH:, :])
    )

    @pl.when(part < 2)
    def _():
        mine[...] = gain[...]
        theirs[...] = gain[...]

    @pl.when(part >= 2)
    def _():
        through = dot3(token[:8, :], jnp.concatenate([amap[...], gain[...]], axis=1))
        for ref, owner in ((mine, part), (theirs, part - 2)):
            rows = pl.ds(pl.multiple_of(owner * ROWS, ROWS), ROWS)
            ref[:ROWS, :] = amap[rows, :]
            ref[ROWS : ROWS + 8, :] = through[:, :CH]
            ref[ROWS + 8 : 2 * ROWS + 8, :] = gain[rows, :]
            ref[2 * ROWS + 8 : 2 * ROWS + 16, :] = through[:, CH:]
            ref[2 * ROWS + 16 :, :] = jnp.zeros((CH - 2 * ROWS - 16, CH), F32)


def rows_kernel(mine, theirs, token, gain_ref, o0, o1, o2, o3, scr, wide):
    right = jnp.where(lax.axis_index("sp_0") < 2, 0, 1)
    scr[right] = mine[...]
    scr[1 - right] = theirs[...]
    final = dot3(scr[1, : ROWS + 8, :], scr[0]) + scr[1, ROWS + 8 : 2 * ROWS + 16, :]
    missing = token[2:3, :] - final[ROWS : ROWS + 1, :]
    wide[:ROWS, :] = final[:ROWS, :] + token[8:, :] * missing
    read = (final[ROWS + 1 : ROWS + 2, :] + token[4:5, :] * missing) / math.sqrt(CH)
    scale = lax.rsqrt(jnp.mean(read * read, axis=-1, keepdims=True) + 1e-06)
    read_rows = jnp.broadcast_to(read * scale * gain_ref[...], (8, CH))
    for k, o in zip(SHIFTS, (o0, o1, o2, o3)):
        y = lax.rem(lax.axis_index("sp_1") + k, 4)
        o[:8, :] = wide[pl.ds(pl.multiple_of(y * 8, 8), 8), :]
        o[8:, :] = read_rows


def finish_kernel(r0, r1, r2, r3, cache_ref, read_ref, scr):
    for k, ref in zip(SHIFTS, (r0, r1, r2, r3)):
        scr[lax.rem(lax.axis_index("sp_1") + 4 - k, 4)] = ref[...]
    for s in range(2):
        for h in range(2):
            cache_ref[s, h] = scr[2 * s + h, :8, :].astype(BF16)
        read_ref[s] = jnp.concatenate([scr[2 * s + h, 8:9, :] for h in range(2)], axis=0).astype(BF16)


def vmem(count):
    return [pl.BlockSpec(memory_space=pltpu.VMEM) for _ in range(count)]


def spread(arrays, axis):
    return [
        lax.ppermute(a, axis, [(i, (i + k) % 4) for i in range(4)]) if k else a
        for k, a in zip(SHIFTS, arrays)
    ]


def swap(array, axis, bit):
    return lax.ppermute(array, axis, [(i, i ^ bit) for i in range(4)])


def shards(
    tokens,
    key_matrix,
    value_matrix,
    gate_matrix,
    decay_matrix,
    gate_bias_offset,
    head_log_decay_rate,
    extra_log_decay,
    next_token_query,
    next_token_key,
    next_token_value,
    next_token_gate,
    readout_norm_gain,
):
    seqs, seg, width = tokens.shape
    cols = key_matrix.shape[1]
    gate_count = gate_matrix.shape[1]
    chunks = seqs * seg // CH
    extra = jnp.transpose(extra_log_decay.reshape(chunks, CH, 2), (0, 2, 1))
    hbm = pl.BlockSpec(memory_space=pltpu.HBM)
    smem = pl.BlockSpec(memory_space=pltpu.SMEM)
    halved = [pltpu.VMEM((2, seg, CH), BF16)] * 2 + [pltpu.VMEM((2, 2 * CH, CH), F32)]
    far2, far3, *kept = pl.pallas_call(
        far_kernel,
        out_shape=[jax.ShapeDtypeStruct((2 * CH, CH), F32)] * 2
        + [
            jax.ShapeDtypeStruct((seg, width), BF16),
            jax.ShapeDtypeStruct((width, cols), BF16),
            jax.ShapeDtypeStruct((width, cols), BF16),
            jax.ShapeDtypeStruct((2 * gate_count, width), BF16),
            jax.ShapeDtypeStruct((chunks, 2, CH), F32),
            jax.ShapeDtypeStruct((8, CH), F32),
        ],
        in_specs=[hbm] * 8,
        out_specs=vmem(8),
        scratch_shapes=[
            pltpu.VMEM((seg, width), BF16),
            pltpu.SMEM(gate_bias_offset.shape, F32),
            pltpu.SMEM(head_log_decay_rate.shape, F32),
            *halved,
            pltpu.SemaphoreType.DMA((10,)),
        ],
        compiler_params=pltpu.CompilerParams(vmem_limit_bytes=24 * 2**20),
        name="far",
    )(
        *(
            pltpu.with_memory_space_constraint(a, pltpu.HBM)
            for a in (
                tokens,
                key_matrix,
                value_matrix,
                gate_matrix.T,
                decay_matrix.T,
                gate_bias_offset,
                head_log_decay_rate,
                extra,
            )
        )
    )
    from2 = swap(far2, "sp_1", 2)
    from3 = swap(far3, "sp_1", 3)
    near = pl.pallas_call(
        near_kernel,
        out_shape=[jax.ShapeDtypeStruct((2 * CH, CH), F32)] * 2,
        in_specs=vmem(6),
        out_specs=vmem(2),
        scratch_shapes=halved,
        compiler_params=pltpu.CompilerParams(vmem_limit_bytes=16 * 2**20),
        cost_estimate=pl.CostEstimate(flops=3 * 10**9, bytes_accessed=10**6, transcendentals=0),
        name="near",
    )
    mine, near1 = near(*kept)
    small = pltpu.CompilerParams(vmem_limit_bytes=8 * 2**20)
    segment = pl.pallas_call(
        segments_kernel,
        out_shape=jax.ShapeDtypeStruct((2 * CH, CH), F32),
        in_specs=vmem(4),
        out_specs=vmem(1)[0],
        scratch_shapes=[pltpu.VMEM((4, 2 * CH, CH), F32)],
        compiler_params=small,
        name="segments",
    )(mine, swap(near1, "sp_1", 1), from2, from3)
    token = pl.pallas_call(
        token_kernel,
        out_shape=jax.ShapeDtypeStruct((8 + ROWS, CH), F32),
        in_specs=[*vmem(3), smem],
        out_specs=vmem(1)[0],
        compiler_params=small,
        name="token",
    )(next_token_query, next_token_key, next_token_value, next_token_gate)
    mine, theirs = pl.pallas_call(
        halves_kernel,
        out_shape=[jax.ShapeDtypeStruct((CH, CH), F32)] * 2,
        in_specs=vmem(3),
        out_specs=vmem(2),
        scratch_shapes=[
            pltpu.VMEM((2, 2 * CH, CH), F32),
            pltpu.VMEM((CH, CH), F32),
            pltpu.VMEM((CH, CH), F32),
        ],
        compiler_params=small,
        name="halves",
    )(segment, swap(segment, "sp_0", 1), token)
    rows = pl.pallas_call(
        rows_kernel,
        out_shape=[jax.ShapeDtypeStruct((16, CH), F32)] * 4,
        in_specs=vmem(4),
        out_specs=vmem(4),
        scratch_shapes=[pltpu.VMEM((2, CH, CH), F32), pltpu.VMEM((ROWS, CH), F32)],
        compiler_params=small,
        name="rows",
    )(mine, swap(theirs, "sp_0", 2), token, readout_norm_gain.reshape(1, CH))
    return pl.pallas_call(
        finish_kernel,
        out_shape=[
            jax.ShapeDtypeStruct((2, 2, 8, CH), BF16),
            jax.ShapeDtypeStruct((2, 2, CH), BF16),
        ],
        in_specs=vmem(4),
        out_specs=vmem(2),
        scratch_shapes=[pltpu.VMEM((4, 16, CH), F32)],
        compiler_params=small,
        name="finish",
    )(*spread(rows, "sp_1"))


def solution(mesh):
    finer = Mesh(
        mesh.devices.reshape(mesh.shape["gr"], 4, 4, mesh.shape["tp"]), ("gr", "sp_0", "sp_1", "tp")
    )
    in_specs = (
        P("gr", SP, None),
        P(None, "tp"),
        P(None, "tp"),
        P(),
        P(),
        P(),
        P(),
        P("gr", SP, "tp"),
        P("gr", "tp", None),
        P("gr", "tp", None),
        P("gr", "tp", None),
        P("gr", "tp"),
        P(),
    )
    out_specs = (P("gr", "tp", SP, None), P("gr", "tp", None))
    return jax.shard_map(
        shards, mesh=finer, in_specs=in_specs, out_specs=out_specs, check_vma=False
    )
```
